512 devices in a mesh: sp: 64 (over z, y), fs: 4 (over x), tp: 2 (over core).
Axes of the slice: x: 4, y: 8, z: 8, core: 2. Of those that a mesh axis runs over, the one named last changes fastest.
Arguments:
- output_gate_logits: bfloat16 [4, 8192, 2048], P('fs', 'sp', 'tp'), may hold values from -6 to 6
- head_input_rows: bfloat16 [4, 8192, 2048], P('fs', 'sp', 'tp'), may hold values from -6 to 6
- group_state_writes: bfloat16 [4, 8192, 512], P('fs', 'sp', 'tp'), may hold values from -6 to 6
- group_state_reads: bfloat16 [4, 8192, 512], P('fs', 'sp', 'tp'), may hold values from -6 to 6
- step_logits: float32 [4, 8192, 32], P('fs', 'sp', 'tp'), may hold values from -5 to 5
- head_step_offset: float32 [32], P('tp'), may hold values from -3.5 to 1
- head_decay_logrates: float32 [32], P('tp'), may hold values from -11 to 0
- decay_extra_spikes: float32 [8192, 32], P('sp', 'tp'), may hold values from -2.1 to 0
- head_input_taps: bfloat16 [4, 2048], P(None, 'tp'), may hold values from -3 to 3
- state_input_taps: bfloat16 [4, 512], P(None, 'tp'), may hold values from -3 to 3
- readout_filter_taps: bfloat16 [4, 512], P(None, 'tp'), may hold values from -3 to 3
- grouped_norm_scale: float32 [2048], P('tp'), may hold values from 0.1 to 1.9
- convolution_outer_gate: bfloat16 [4, 8192, 1024], P('fs', 'sp', 'tp'), may hold values from -6 to 6
- convolution_inner_gate: bfloat16 [4, 8192, 1024], P('fs', 'sp', 'tp'), may hold values from -6 to 6
- convolution_value_rows: bfloat16 [4, 8192, 1024], P('fs', 'sp', 'tp'), may hold values from -6 to 6
- gated_filter_taps: bfloat16 [3, 1024], P(None, 'tp'), may hold values from -3.5 to 3.5
- state_output_rows: bfloat16 [2048, 2048], P('tp', 'fs'), may hold values from -0.09375 to 0.09375
- convolution_output_rows: bfloat16 [1024, 2048], P('tp', 'fs'), may hold values from -0.125 to 0.125
Outputs:
- layer_out: bfloat16 [4, 8192, 2048], P('tp', 'sp', 'fs')
The draws below stay inside these ranges and needn't reach their ends.
All inputs are finite; a program needn't handle non-finite values.
Results may differ from the reference program's by a relative error of at most 0.012.
Values may be sent and summed in bfloat16 or wider, within the bound.
No kernel may reach another device: no remote copies, remote signals or barrier semaphores. Data moves between devices by JAX's collectives and lax.ppermute only.
A program may use at most 64 MiB of HBM per device.

```python
import jax
import jax.numpy as jnp
from jax import lax

D = 2048
HEADS = 32
HEAD_DIM = 64
GROUPS = 4
STATE = 128
CHANNELS = 1024
BLOCK = 128
SSD_TAPS = 4
CONV_TAPS = 3
TOK_DEV = 128
LENGTH = 8192
SEQS = 4


def slow_heads(key):
    share = HEADS // 2
    order = jax.random.permutation(jax.random.fold_in(key, 11), HEADS)
    return order < share


def draw_head_decay_logrates(key, part):
    slow = slow_heads(key)
    spread = jax.random.uniform(jax.random.fold_in(key, 12), (HEADS,), jnp.float32)
    slow_rate = (0.2 + 0.6 * spread) / (0.07 * LENGTH)
    fast_rate = 0.01 * jnp.exp(spread * jnp.log(3.3))
    return jnp.log(jnp.where(slow, slow_rate, fast_rate)).astype(jnp.float32)


def draw_head_step_offset(key, part):
    slow = slow_heads(key)
    spread = jax.random.uniform(jax.random.fold_in(key, 13), (HEADS,), jnp.float32)
    return jnp.where(slow, spread - 3.5, spread).astype(jnp.float32)


def draw_step_logits(key, part):
    blocks = LENGTH // TOK_DEV
    quiet_span = max(1, blocks // 4)
    noise = jnp.clip(jax.random.normal(jax.random.fold_in(key, 22), (SEQS, LENGTH, HEADS), jnp.float32), -4.0, 4.0)
    offset = jax.random.uniform(jax.random.fold_in(key, 23), (SEQS, blocks, 1, HEADS), jnp.float32, -1.0, 1.0)
    lowered = jax.random.uniform(jax.random.fold_in(key, 24), (SEQS, blocks, 1, HEADS), jnp.float32, -5.0, -3.5)
    begin = jax.random.randint(jax.random.fold_in(key, 25), (SEQS, 1), 0, blocks - quiet_span + 1)
    places = jnp.arange(blocks, dtype=jnp.int32)[None, :]
    quiet = jnp.logical_and(places >= begin, places < begin + quiet_span)
    offset = jnp.where(quiet[:, :, None, None], lowered, offset)
    factor = jnp.where(quiet[:, :, None, None], 0.5, 1.0) * jnp.ones((SEQS, blocks, 1, HEADS), jnp.float32)
    offset = jnp.broadcast_to(offset, (SEQS, blocks, TOK_DEV, HEADS)).reshape(SEQS, LENGTH, HEADS)
    factor = jnp.broadcast_to(factor, (SEQS, blocks, TOK_DEV, HEADS)).reshape(SEQS, LENGTH, HEADS)
    return jnp.clip(noise * factor + offset, -5.0, 5.0).astype(jnp.float32)


def draw_decay_extra_spikes(key, part):
    spots = jax.random.randint(jax.random.fold_in(key, 31), (3,), 0, LENGTH)
    sizes = -jax.random.uniform(jax.random.fold_in(key, 32), (3, HEADS), jnp.float32, 0.22, 0.69)
    places = jnp.arange(LENGTH, dtype=jnp.int32)
    match = places[:, None] == spots[None, :]
    return jnp.sum(jnp.where(match[:, :, None], sizes[None], 0.0), axis=1).astype(jnp.float32)


def steps_of(rng, dims, cuts, smallest, top_value):
    factor_of = 1.0
    for axis_at, shards_of in cuts:
        draws = jax.random.uniform(jax.random.fold_in(jax.random.fold_in(rng, 6), axis_at), (shards_of,), jnp.float32, smallest / len(cuts), top_value / len(cuts))
        factor_of = factor_of * jnp.repeat(jnp.exp(draws), dims[axis_at] // shards_of).reshape((-1,) + (1,) * (len(dims) - 1 - axis_at))
    return factor_of


def scatter_about(stream_key, shape, deviation, most, cuts=(), kind=jnp.bfloat16):
    result = jax.random.normal(stream_key, shape, jnp.float32) * deviation
    if len(cuts) > 0:
        result = steps_of(stream_key, shape, cuts, -0.22, 0.18) * result
    return jnp.clip(result, min=-most, max=most).astype(kind)


def setup_inputs(seed: int = 0) -> dict:
    splits = jax.random.split(jax.random.key(seed), 19)
    output_gate_logits = scatter_about(splits[0], (SEQS, LENGTH, HEADS * HEAD_DIM), 1.0, 6.0, ((0, 4), (1, 64), (2, 2)))
    head_input_rows = scatter_about(splits[1], (SEQS, LENGTH, HEADS * HEAD_DIM), 1.0, 6.0, ((0, 4), (1, 64), (2, 2)))
    group_state_writes = scatter_about(splits[2], (SEQS, LENGTH, GROUPS * STATE), 1.0, 6.0, ((0, 4), (1, 64), (2, 2)))
    group_state_reads = scatter_about(splits[3], (SEQS, LENGTH, GROUPS * STATE), 1.0, 6.0, ((0, 4), (1, 64), (2, 2)))
    step_logits = draw_step_logits(jax.random.fold_in(splits[18], 71), 0)
    head_step_offset = draw_head_step_offset(jax.random.fold_in(splits[18], 71), 0)
    head_decay_logrates = draw_head_decay_logrates(jax.random.fold_in(splits[18], 71), 0)
    decay_extra_spikes = draw_decay_extra_spikes(jax.random.fold_in(splits[18], 71), 0)
    head_input_taps = scatter_about(splits[8], (SSD_TAPS, HEADS * HEAD_DIM), SSD_TAPS ** -0.5, 3.0, ((1, 2),))
    state_input_taps = scatter_about(splits[9], (SSD_TAPS, GROUPS * STATE), SSD_TAPS ** -0.5, 3.0, ((1, 2),))
    readout_filter_taps = scatter_about(splits[10], (SSD_TAPS, GROUPS * STATE), SSD_TAPS ** -0.5, 3.0, ((1, 2),))
    grouped_norm_scale = jnp.clip(1.0 + 0.18 * jax.random.normal(splits[11], (HEADS * HEAD_DIM,), jnp.float32), 0.1, 1.9)
    convolution_outer_gate = scatter_about(splits[12], (SEQS, LENGTH, CHANNELS), 1.0, 6.0, ((0, 4), (1, 64), (2, 2)))
    convolution_inner_gate = scatter_about(splits[13], (SEQS, LENGTH, CHANNELS), 1.0, 6.0, ((0, 4), (1, 64), (2, 2)))
    convolution_value_rows = scatter_about(splits[14], (SEQS, LENGTH, CHANNELS), 1.0, 6.0, ((0, 4), (1, 64), (2, 2)))
    gated_filter_taps = scatter_about(splits[15], (CONV_TAPS, CHANNELS), CONV_TAPS ** -0.5, 3.5, ((1, 2),))
    state_output_rows = scatter_about(splits[16], (HEADS * HEAD_DIM, D), (2 * HEADS * HEAD_DIM) ** -0.5, 0.09375, ((0, 2), (1, 4)))
    convolution_output_rows = scatter_about(splits[17], (CHANNELS, D), (2 * CHANNELS) ** -0.5, 0.125, ((0, 2), (1, 4)))
    return dict(output_gate_logits=output_gate_logits, head_input_rows=head_input_rows, group_state_writes=group_state_writes, group_state_reads=group_state_reads, step_logits=step_logits, head_step_offset=head_step_offset, head_decay_logrates=head_decay_logrates, decay_extra_spikes=decay_extra_spikes, head_input_taps=head_input_taps, state_input_taps=state_input_taps, readout_filter_taps=readout_filter_taps, grouped_norm_scale=grouped_norm_scale, convolution_outer_gate=convolution_outer_gate, convolution_inner_gate=convolution_inner_gate, convolution_value_rows=convolution_value_rows, gated_filter_taps=gated_filter_taps, state_output_rows=state_output_rows, convolution_output_rows=convolution_output_rows)


EPS = 1e-06
HIGH = lax.Precision.HIGHEST

def causal_filter(stream, kernel, before):
    span = kernel.shape[0]
    length = stream.shape[1]
    padded = jnp.concatenate([before, stream], axis=1)
    total = padded[:, 0:length] * kernel[0]
    for offset in range(1, span):
        total = total + padded[:, offset:offset + length] * kernel[offset]
    return total

def block_scan(driven, decay, writes, reads):
    batch, length, groups, ratio, channels = driven.shape
    entries = writes.shape[-1]
    count = length // BLOCK

    def split(array):
        shaped = array.reshape((batch, count, BLOCK) + array.shape[2:])
        return jnp.moveaxis(shaped, 1, 0)
    causal = jnp.tril(jnp.ones((BLOCK, BLOCK), dtype=bool))

    def advance(carry, pieces):
        drive, fall, write, read = pieces
        rising = jnp.cumsum(fall, axis=1)
        scores = jnp.einsum('blgn,bsgn->bgls', read, write, precision=HIGH)
        gaps = rising[:, :, None] - rising[:, None, :]
        weights = jnp.exp(jnp.where(causal[None, :, :, None, None], gaps, -jnp.inf))
        inside = jnp.einsum('bgls,blsgr,bsgrp->blgrp', scores, weights, drive, precision=HIGH)
        earlier = jnp.einsum('blgn,bgrpn->blgrp', read, carry, precision=HIGH) * jnp.exp(rising)[..., None]
        remain = jnp.exp(rising[:, -1:] - rising)
        fresh = jnp.einsum('bsgn,bsgr,bsgrp->bgrpn', write, remain, drive, precision=HIGH)
        carry = carry * jnp.exp(rising[:, -1])[..., None, None] + fresh
        return (carry, inside + earlier)
    start = jnp.zeros((batch, groups, ratio, channels, entries), jnp.float32)
    final, blocks = lax.scan(advance, start, (split(driven), split(decay), split(writes), split(reads)))
    return (final, jnp.moveaxis(blocks, 0, 1).reshape(driven.shape))

def reference(output_gate_logits, head_input_rows, group_state_writes, group_state_reads, step_logits, head_step_offset, head_decay_logrates, decay_extra_spikes, head_input_taps, state_input_taps, readout_filter_taps, grouped_norm_scale, convolution_outer_gate, convolution_inner_gate, convolution_value_rows, gated_filter_taps, state_output_rows, convolution_output_rows):
    ratio = HEADS // GROUPS

    def one_sequence(streams):
        gate, inputs, writes_raw, reads_raw, raw_step, outer, inner, values = streams
        length = inputs.shape[0]
        reach = head_input_taps.shape[0] - 1
        short = gated_filter_taps.shape[0] - 1
        filtered_input = jax.nn.silu(causal_filter(inputs[None].astype(jnp.float32), head_input_taps.astype(jnp.float32), jnp.zeros((1, reach, inputs.shape[1]), jnp.float32)))
        filtered_writes = jax.nn.silu(causal_filter(writes_raw[None].astype(jnp.float32), state_input_taps.astype(jnp.float32), jnp.zeros((1, reach, writes_raw.shape[1]), jnp.float32)))
        filtered_reads = jax.nn.silu(causal_filter(reads_raw[None].astype(jnp.float32), readout_filter_taps.astype(jnp.float32), jnp.zeros((1, reach, reads_raw.shape[1]), jnp.float32)))
        head_step_length = jax.nn.softplus(raw_step[None] + head_step_offset)
        decay_logarithm = decay_extra_spikes[None] - head_step_length * jnp.exp(head_decay_logrates)
        driven = (filtered_input.reshape(1, length, HEADS, HEAD_DIM) * head_step_length[..., None]).reshape(1, length, GROUPS, ratio, HEAD_DIM)
        final, state_output = block_scan(driven, decay_logarithm.reshape(1, length, GROUPS, ratio), filtered_writes.reshape(1, length, GROUPS, STATE), filtered_reads.reshape(1, length, GROUPS, STATE))
        gated = state_output.reshape(1, length, HEADS * HEAD_DIM) * jax.nn.silu(gate[None].astype(jnp.float32))
        grouped = gated.reshape(1, length, GROUPS, ratio * HEAD_DIM)
        normed = grouped * lax.rsqrt(lax.optimization_barrier(jnp.mean(grouped * grouped, axis=-1, keepdims=True)) + EPS)
        state_branch = (normed.reshape(1, length, HEADS * HEAD_DIM) * grouped_norm_scale).astype(jnp.bfloat16)
        product = inner[None].astype(jnp.float32) * values[None].astype(jnp.float32)
        filtered = causal_filter(product, gated_filter_taps.astype(jnp.float32), jnp.zeros((1, short, inner.shape[1]), jnp.float32))
        conv_branch = (outer[None].astype(jnp.float32) * filtered).astype(jnp.bfloat16)
        mixed = jnp.dot(state_branch[0], state_output_rows, preferred_element_type=jnp.float32) + jnp.dot(conv_branch[0], convolution_output_rows, preferred_element_type=jnp.float32)
        return mixed.astype(jnp.bfloat16)
    return lax.map(one_sequence, (output_gate_logits, head_input_rows, group_state_writes, group_state_reads, step_logits, convolution_outer_gate, convolution_inner_gate, convolution_value_rows))
```

```python
import jax
import jax.numpy as jnp
from jax import lax
from jax.experimental import pallas as pl
from jax.experimental.pallas import tpu as pltpu
from jax.sharding import PartitionSpec as P

EPS = 1e-06
F32 = jnp.float32
BF16 = jnp.bfloat16
STATE = 128
LANES = 128
HEAD_DIM = 64
EXTRA = 8
RIM = 8
HEAD = 16


def whole(shape):
    return pl.BlockSpec(shape, lambda *_: (0,) * len(shape))


HBM = pl.BlockSpec(memory_space=pltpu.HBM)


def call(kernel, outs, ins, far=0, scratch=(), flops=50_000_000):
    ins = [pltpu.with_memory_space_constraint(a, pltpu.HBM) for a in ins[:far]] + list(ins[far:])
    return pl.pallas_call(
        kernel,
        grid=(1,),
        in_specs=[HBM] * far + [whole(a.shape) for a in ins[far:]],
        out_specs=[whole(o.shape) for o in outs],
        out_shape=outs,
        scratch_shapes=scratch,
        compiler_params=pltpu.CompilerParams(vmem_limit_bytes=24 * 1024 * 1024),
        cost_estimate=pl.CostEstimate(flops=flops, bytes_accessed=2_000_000, transcendentals=0),
    )(*ins)


def vmem(shape, dtype=F32):
    return pltpu.VMEM(shape, dtype)


def sems(count):
    return pltpu.SemaphoreType.DMA((count,))


def silu(v):
    return v / (1.0 + jnp.exp(-v))


def pair_lanes(cols, q, rows):
    low = lax.broadcasted_iota(jnp.int32, (rows, LANES), 1) < HEAD_DIM
    first = jnp.broadcast_to(cols[:, 2 * q : 2 * q + 1], (rows, LANES))
    second = jnp.broadcast_to(cols[:, 2 * q + 1 : 2 * q + 2], (rows, LANES))
    return jnp.where(low, first, second)


def fetch(pairs, sems):
    copies = [pltpu.make_async_copy(src, dst, sems.at[k]) for k, (src, dst) in enumerate(pairs)]
    for copy in copies:
        copy.start()
    return copies


def rims_kernel(x_ref, w_ref, r_ref, i_ref, v_ref, out_ref, sems):
    at = 0
    pairs = []
    for ref in (x_ref, w_ref, r_ref, i_ref, v_ref):
        length, width = ref.shape[1:]
        pairs.append((ref.at[0, pl.ds(length - RIM, RIM)], out_ref.at[:, pl.ds(at, width)]))
        at += width
    for copy in fetch(pairs, sems):
        copy.wait()


def filtered(rows, taps, rim, pad_ref):
    length, width = rows.shape
    span = taps.shape[0]
    if rim is None:
        rim = jnp.zeros((RIM, width), F32)
    pad_ref[0:RIM, 0:width] = rim
    pad_ref[RIM : RIM + length, 0:width] = rows
    total = rows * taps[span - 1 : span, :]
    for k in range(span - 1):
        back = span - 1 - k
        total = total + pad_ref[RIM - back : RIM - back + length, 0:width] * taps[k : k + 1, :]
    return total


def column(row):
    size = row.shape[1]
    here = lax.broadcasted_iota(jnp.int32, (size, size), 0) == lax.broadcasted_iota(
        jnp.int32, (size, size), 1
    )
    return jnp.sum(jnp.where(here, jnp.broadcast_to(row, (size, size)), 0.0), axis=1, keepdims=True)


def prepare_kernel(
    x_hbm, w_hbm, xt_hbm, wt_hbm, step_hbm, spike_hbm, off_hbm, rate_hbm,
    xdt_ref, weighted_ref, writes_ref, head_ref, xt_ref, wt_ref, dt_ref, rise_ref, rise_t_ref, remain_ref,
    x_ref, w_ref, step_ref, spike_ref, off_ref, rate_ref, pad_ref, sems,
):
    width = x_hbm.shape[2]
    narrow = w_hbm.shape[2]
    copies = fetch(
        (
            (step_hbm.at[0], step_ref),
            (spike_hbm, spike_ref),
            (off_hbm, off_ref),
            (rate_hbm, rate_ref),
            (w_hbm.at[0], w_ref),
            (wt_hbm, wt_ref),
            (x_hbm.at[0], x_ref),
            (xt_hbm, xt_ref),
            (x_hbm.at[0, pl.ds(0, HEAD)], head_ref.at[:, pl.ds(0, width)]),
            (w_hbm.at[0, pl.ds(0, HEAD)], head_ref.at[:, pl.ds(width, narrow)]),
        ),
        sems,
    )
    for copy in copies[:4]:
        copy.wait()
    heads, length = step_ref.shape
    raw = step_ref[...] + column(off_ref[...])
    dt_t = jnp.maximum(raw, 0.0) + jnp.log1p(jnp.exp(-jnp.abs(raw)))
    fall_t = spike_ref[...] - dt_t * column(jnp.exp(rate_ref[...]))
    row = lax.broadcasted_iota(jnp.int32, (length, length), 0)
    col = lax.broadcasted_iota(jnp.int32, (length, length), 1)
    rise_t = jnp.dot(
        fall_t, (row <= col).astype(F32), precision=lax.Precision.HIGHEST, preferred_element_type=F32
    )
    rise_t_ref[...] = rise_t
    tall = jnp.concatenate([rise_t, dt_t, jnp.zeros((LANES - 2 * heads, length), F32)], axis=0)
    wide = jnp.transpose(tall)
    rise = wide[:, 0:heads]
    dt = wide[:, heads : 2 * heads]
    rise_ref[...] = rise
    dt_ref[...] = dt
    remain = jnp.exp(jnp.minimum(rise[length - 1 : length, :] - rise, 0.0))
    remain_ref[...] = remain
    copies[4].wait()
    copies[5].wait()
    for c in range(0, narrow, STATE):
        cols = slice(c, c + STATE)
        writes_ref[:, cols] = silu(
            filtered(w_ref[:, cols].astype(F32), wt_ref[:, cols].astype(F32), None, pad_ref)
        ).astype(BF16)
    copies[6].wait()
    copies[7].wait()
    for q in range(width // LANES):
        cols = slice(q * LANES, (q + 1) * LANES)
        x = silu(filtered(x_ref[:, cols].astype(F32), xt_ref[:, cols].astype(F32), None, pad_ref))
        x = x * pair_lanes(dt, q, length)
        xdt_ref[:, cols] = x.astype(BF16)
        weighted_ref[:, cols] = (x * pair_lanes(remain, q, length)).astype(BF16)
    copies[8].wait()
    copies[9].wait()


def state_kernel(
    rim_ref, xdt_in, weighted_in, writes_in, head_ref, xt_ref, wt_ref, dt_ref, rise_ref, remain_ref,
    pay_ref, xdt_ref, writes_ref, pad_ref,
):
    length, width = xdt_in.shape
    groups = writes_in.shape[1] // STATE
    per_group = width // LANES // groups
    sub = lax.broadcasted_iota(jnp.int32, (EXTRA, LANES), 0)
    total = rise_ref[length - 1 : length, :]
    dt = dt_ref[0:HEAD, :]
    remain = remain_ref[0:HEAD, :]
    blocks = STATE // 16
    for g in range(groups):
        cols = slice(g * STATE, (g + 1) * STATE)
        spot = slice(width + g * STATE, width + (g + 1) * STATE)
        first = silu(
            filtered(head_ref[:, spot].astype(F32), wt_ref[:, cols].astype(F32), rim_ref[:, spot].astype(F32), pad_ref)
        ).astype(BF16)
        write = jnp.concatenate([first, writes_in[HEAD:, cols]], axis=0)
        writes_ref[:, cols] = write
        write_t = jnp.transpose(write.astype(F32)).astype(BF16)
        for q in range(g * per_group, (g + 1) * per_group):
            cols = slice(q * LANES, (q + 1) * LANES)
            x = silu(
                filtered(head_ref[:, cols].astype(F32), xt_ref[:, cols].astype(F32), rim_ref[:, cols].astype(F32), pad_ref)
            )
            x = x * pair_lanes(dt, q, HEAD)
            xdt_ref[0:HEAD, cols] = x.astype(BF16)
            xdt_ref[HEAD:, cols] = xdt_in[HEAD:, cols]
            x = (x * pair_lanes(remain, q, HEAD)).astype(BF16)
            weighted = jnp.concatenate([x, weighted_in[HEAD:, cols]], axis=0)
            state = jnp.dot(write_t, weighted, preferred_element_type=F32)
            pay_ref[q * blocks : (q + 1) * blocks, 0:16, :] = state.reshape(blocks, 16, LANES).astype(BF16)
            t = pair_lanes(total, q, 1)
            hi = t.astype(BF16).astype(F32)
            mid = (t - hi).astype(BF16).astype(F32)
            lo = t - hi - mid
            terms = jnp.where(sub == 0, hi, jnp.where(sub == 1, mid, jnp.where(sub == 2, lo, 0.0))).astype(BF16)
            pay_ref[q * blocks : (q + 1) * blocks, 16 : 16 + EXTRA, :] = jnp.broadcast_to(terms[None], (blocks, EXTRA, LANES))


def inside_kernel(
    r_hbm, i_hbm, v_hbm, o_hbm, rt_hbm, ct_hbm, gate_hbm, scale_hbm,
    rim_ref, xdt_ref, writes_ref, rise_ref, rise_t_ref,
    inside_ref, reads_ref, conv_ref, open_ref, scale_ref,
    r_ref, i_ref, v_ref, o_ref, rt_ref, ct_ref, gate_ref, pad_ref, sems,
):
    copies = fetch(
        (
            (r_hbm.at[0], r_ref),
            (rt_hbm, rt_ref),
            (i_hbm.at[0], i_ref),
            (v_hbm.at[0], v_ref),
            (o_hbm.at[0], o_ref),
            (ct_hbm, ct_ref),
            (gate_hbm.at[0], gate_ref),
            (scale_hbm, scale_ref),
        ),
        sems,
    )
    length, width = xdt_ref.shape
    groups = writes_ref.shape[1] // STATE
    per_group = width // LANES // groups
    row = lax.broadcasted_iota(jnp.int32, (length, length), 0)
    col = lax.broadcasted_iota(jnp.int32, (length, length), 1)
    causal = row >= col
    rise = rise_ref[...]
    rise_t = rise_t_ref[...]
    low = lax.broadcasted_iota(jnp.int32, (length, LANES), 1) < HEAD_DIM
    base = width + groups * STATE
    copies[0].wait()
    copies[1].wait()
    for g in range(groups):
        cols = slice(g * STATE, (g + 1) * STATE)
        spot = slice(base + g * STATE, base + (g + 1) * STATE)
        read = silu(
            filtered(r_ref[:, cols].astype(F32), rt_ref[:, cols].astype(F32), rim_ref[:, spot].astype(F32), pad_ref)
        ).astype(BF16)
        reads_ref[:, cols] = read
        scores = lax.dot_general(
            read, writes_ref[:, cols], (((1,), (1,)), ((), ())), preferred_element_type=F32
        )
        scores = jnp.where(causal, scores, 0.0)
        for q in range(g * per_group, (g + 1) * per_group):
            both = []
            for h in (2 * q, 2 * q + 1):
                gap = jnp.minimum(rise[:, h : h + 1] - rise_t[h : h + 1, :], 0.0)
                both.append((scores * jnp.exp(gap)).astype(BF16))
            x = xdt_ref[:, q * LANES : (q + 1) * LANES]
            zero = jnp.zeros_like(x)
            stacked = jnp.concatenate([jnp.where(low, x, zero), jnp.where(low, zero, x)], axis=0)
            inside_ref[:, q * LANES : (q + 1) * LANES] = jnp.dot(
                jnp.concatenate(both, axis=1), stacked, preferred_element_type=F32
            )
    for copy in copies[2:]:
        copy.wait()
    for c in range(0, width, LANES):
        open_ref[:, c : c + LANES] = silu(gate_ref[:, c : c + LANES].astype(F32))
    base = base + groups * STATE
    wide = i_ref.shape[1]
    for c in range(0, wide, LANES):
        cols = slice(c, c + LANES)
        product = i_ref[:, cols].astype(F32) * v_ref[:, cols].astype(F32)
        rim = rim_ref[:, base + c : base + c + LANES].astype(F32) * rim_ref[
            :, base + wide + c : base + wide + c + LANES
        ].astype(F32)
        total = filtered(product, ct_ref[:, cols].astype(F32), rim, pad_ref)
        conv_ref[:, cols] = (o_ref[:, cols].astype(F32) * total).astype(BF16)


def scan_kernel(in_ref, out_ref):
    members = in_ref.shape[0]
    carry = jnp.zeros((16, LANES), F32)
    for j in range(members):
        out_ref[j] = carry.astype(BF16)
        if j + 1 < members:
            t = in_ref[j, 16 : 16 + EXTRA, :].astype(F32)
            decay = jnp.exp(t[0:1, :] + t[1:2, :] + t[2:3, :])
            carry = carry * decay + in_ref[j, 0:16, :].astype(F32)


def gate_kernel(p_ref, reads_ref, rise_ref, inside_ref, open_ref, scale_ref, conv_ref, out_ref):
    length, width = inside_ref.shape
    groups = reads_ref.shape[1] // STATE
    per_group = width // LANES // groups
    kept = jnp.exp(rise_ref[...])
    blocks = STATE // 16
    copies = out_ref.shape[0]
    for g in range(groups):
        read = reads_ref[:, g * STATE : (g + 1) * STATE]
        squares = jnp.zeros((length, LANES), F32)
        gated = []
        for q in range(g * per_group, (g + 1) * per_group):
            cols = slice(q * LANES, (q + 1) * LANES)
            before = p_ref[q * blocks : (q + 1) * blocks].reshape(STATE, LANES)
            carried = jnp.dot(read, before, preferred_element_type=F32)
            y = inside_ref[:, cols] + carried * pair_lanes(kept, q, length)
            y = y * open_ref[:, cols]
            squares = squares + y * y
            gated.append(y)
        mean = jnp.sum(squares, axis=1, keepdims=True) * (1.0 / (per_group * LANES))
        inverse = lax.rsqrt(mean + EPS)
        for k, q in enumerate(range(g * per_group, (g + 1) * per_group)):
            cols = slice(q * LANES, (q + 1) * LANES)
            value = (gated[k] * inverse * scale_ref[:, cols]).astype(BF16)
            for c in range(copies):
                out_ref[c, :, cols] = value
    for c in range(copies):
        out_ref[c, :, width:] = conv_ref[...]


def project_kernel(half_ref, a_ref, s_ref, c_ref, out_ref):
    seqs, length, depth = a_ref.shape
    width = s_ref.shape[0]
    start = half_ref[0]
    for k in range(seqs // 2):
        rows = a_ref[start + k]
        out_ref[k] = (
            jnp.dot(rows[:, :width], s_ref[...], preferred_element_type=F32)
            + jnp.dot(rows[:, width:], c_ref[...], preferred_element_type=F32)
        ).astype(out_ref.dtype)


def project(half, rows, s, c, dtype):
    seqs, length, _ = rows.shape
    out = jax.ShapeDtypeStruct((seqs // 2, length, s.shape[1]), dtype)
    ins = (half, rows, s, c)
    return pl.pallas_call(
        project_kernel,
        grid=(1,),
        in_specs=[pl.BlockSpec(memory_space=pltpu.SMEM)] + [whole(a.shape) for a in ins[1:]],
        out_specs=whole(out.shape),
        out_shape=out,
        compiler_params=pltpu.CompilerParams(vmem_limit_bytes=24 * 1024 * 1024),
        cost_estimate=pl.CostEstimate(
            flops=400_000_000, bytes_accessed=2_000_000, transcendentals=0
        ),
    )(*ins)


def merge_kernel(kept_ref, got_ref, out_ref):
    out_ref[...] = (kept_ref[...] + got_ref[...].astype(F32)).astype(BF16)


def per_device(
    output_gate_logits,
    head_input_rows,
    group_state_writes,
    group_state_reads,
    step_logits,
    head_step_offset,
    head_decay_logrates,
    decay_extra_spikes,
    head_input_taps,
    state_input_taps,
    readout_filter_taps,
    grouped_norm_scale,
    convolution_outer_gate,
    convolution_inner_gate,
    convolution_value_rows,
    gated_filter_taps,
    state_output_rows,
    convolution_output_rows,
):
    sds = jax.ShapeDtypeStruct
    _, length, width = head_input_rows.shape
    heads = step_logits.shape[2]
    narrow = group_state_writes.shape[2]
    wide = convolution_inner_gate.shape[2]
    members = lax.axis_size("sp")
    copies = lax.axis_size("fs")
    ends = (
        head_input_rows,
        group_state_writes,
        group_state_reads,
        convolution_inner_gate,
        convolution_value_rows,
    )
    all_width = sum(a.shape[2] for a in ends)
    rims = call(rims_kernel, [sds((RIM, all_width), BF16)], ends, 5, [sems(5)], 1000)[0]
    before = lax.ppermute(rims, "sp", [(k, k + 1) for k in range(members - 1)])
    ins = (
        head_input_rows, group_state_writes, head_input_taps, state_input_taps,
        jnp.swapaxes(step_logits, 1, 2), decay_extra_spikes.T,
        head_step_offset[None], head_decay_logrates[None],
    )
    outs = [
        sds((length, width), BF16),
        sds((length, width), BF16),
        sds((length, narrow), BF16),
        sds((HEAD, width + narrow), BF16),
        sds(head_input_taps.shape, BF16),
        sds(state_input_taps.shape, BF16),
        sds((length, heads), F32),
        sds((length, heads), F32),
        sds((heads, length), F32),
        sds((length, heads), F32),
    ]
    pad = vmem((RIM + length, LANES))
    scratch = [
        vmem((length, width), BF16),
        vmem((length, narrow), BF16),
        vmem((heads, length)),
        vmem((heads, length)),
        vmem((1, heads)),
        vmem((1, heads)),
        pad,
        sems(10),
    ]
    xdt, weighted, writes, head, xt, wt, dt, rise, rise_t, remain = call(
        prepare_kernel, outs, ins, 8, scratch
    )
    ins = (before, xdt, weighted, writes, head, xt, wt, dt, rise, remain)
    outs = [
        sds((members, 16 + EXTRA, LANES), BF16),
        sds((length, width), BF16),
        sds((length, narrow), BF16),
    ]
    payload, xdt, writes = call(state_kernel, outs, ins, 0, [pad])
    gathered = lax.all_to_all(payload, "sp", 0, 0, tiled=True)
    ins = (
        group_state_reads, convolution_inner_gate, convolution_value_rows, convolution_outer_gate,
        readout_filter_taps, gated_filter_taps, output_gate_logits, grouped_norm_scale[None],
        before, xdt, writes, rise, rise_t,
    )
    outs = [
        sds((length, width), F32),
        sds((length, narrow), BF16),
        sds((length, wide), BF16),
        sds((length, width), F32),
        sds((1, width), F32),
    ]
    scratch = [
        vmem((length, narrow), BF16),
        vmem((length, wide), BF16),
        vmem((length, wide), BF16),
        vmem((length, wide), BF16),
        vmem(readout_filter_taps.shape, BF16),
        vmem(gated_filter_taps.shape, BF16),
        vmem((length, width), BF16),
        pad,
        sems(8),
    ]
    inside, reads, conv, opened, scale = call(inside_kernel, outs, ins, 8, scratch)
    prefixes = call(scan_kernel, [sds((members, 16, LANES), BF16)], (gathered,))[0]
    incoming = lax.all_to_all(prefixes, "sp", 0, 0, tiled=True)
    ins = (incoming, reads, rise, inside, opened, scale, conv)
    joined = call(gate_kernel, [sds((copies, length, width + wide), BF16)], ins)[0]
    rows = lax.all_to_all(joined, "fs", 0, 0, tiled=True)
    core = lax.axis_index("tp")
    seqs = copies
    mine = (core * (seqs // 2)).astype(jnp.int32)[None]
    theirs = ((1 - core) * (seqs // 2)).astype(jnp.int32)[None]
    sent = project(theirs, rows, state_output_rows, convolution_output_rows, BF16)
    got = lax.ppermute(sent, "tp", [(0, 1), (1, 0)])
    kept = project(mine, rows, state_output_rows, convolution_output_rows, F32)
    return call(merge_kernel, [sds(got.shape, BF16)], (kept, got))[0]


def solution(mesh):
    return jax.shard_map(
        per_device,
        mesh=mesh,
        in_specs=(
            P("fs", "sp", "tp"),
            P("fs", "sp", "tp"),
            P("fs", "sp", "tp"),
            P("fs", "sp", "tp"),
            P("fs", "sp", "tp"),
            P("tp"),
            P("tp"),
            P("sp", "tp"),
            P(None, "tp"),
            P(None, "tp"),
            P(None, "tp"),
            P("tp"),
            P("fs", "sp", "tp"),
            P("fs", "sp", "tp"),
            P("fs", "sp", "tp"),
            P(None, "tp"),
            P("tp", "fs"),
            P("tp", "fs"),
        ),
        out_specs=P("tp", "sp", "fs"),
        check_vma=False,
    )
```

```python
import jax
import jax.numpy as jnp
from jax import lax
from jax.experimental import pallas as pl
from jax.experimental.pallas import tpu as pltpu
from jax.sharding import PartitionSpec as P

EPS = 1e-06
F32 = jnp.float32
BF16 = jnp.bfloat16
STATE = 128
LANES = 128
HEAD_DIM = 64
EXTRA = 8
PAD = 8
RIM = 4
HEAD = 16
FIRST_OUT = 52
FIRST_BACK = 52


def whole(shape):
    return pl.BlockSpec(shape, lambda *_: (0,) * len(shape))


HBM = pl.BlockSpec(memory_space=pltpu.HBM)


def call(kernel, outs, ins, far=0, scratch=(), flops=50_000_000):
    ins = [pltpu.with_memory_space_constraint(a, pltpu.HBM) for a in ins[:far]] + list(ins[far:])
    return pl.pallas_call(
        kernel,
        grid=(1,),
        in_specs=[HBM] * far + [whole(a.shape) for a in ins[far:]],
        out_specs=[whole(o.shape) for o in outs],
        out_shape=outs,
        scratch_shapes=scratch,
        compiler_params=pltpu.CompilerParams(vmem_limit_bytes=24 * 1024 * 1024),
        cost_estimate=pl.CostEstimate(flops=flops, bytes_accessed=2_000_000, transcendentals=0),
    )(*ins)


def vmem(shape, dtype=F32):
    return pltpu.VMEM(shape, dtype)


def sems(count):
    return pltpu.SemaphoreType.DMA((count,))


def silu(v):
    return v / (1.0 + jnp.exp(-v))


def pair_lanes(cols, q, rows):
    low = lax.broadcasted_iota(jnp.int32, (rows, LANES), 1) < HEAD_DIM
    first = jnp.broadcast_to(cols[:, 2 * q : 2 * q + 1], (rows, LANES))
    second = jnp.broadcast_to(cols[:, 2 * q + 1 : 2 * q + 2], (rows, LANES))
    return jnp.where(low, first, second)


def fetch(pairs, sems):
    copies = [pltpu.make_async_copy(src, dst, sems.at[k]) for k, (src, dst) in enumerate(pairs)]
    for copy in copies:
        copy.start()
    return copies


def rims_kernel(x_ref, w_ref, r_ref, i_ref, v_ref, out_ref, rows_ref, sems):
    at = 0
    pairs = []
    for ref in (x_ref, w_ref, r_ref, i_ref, v_ref):
        length, width = ref.shape[1:]
        pairs.append((ref.at[0, pl.ds(length - PAD, PAD)], rows_ref.at[:, pl.ds(at, width)]))
        at += width
    for copy in fetch(pairs, sems):
        copy.wait()
    out_ref[...] = rows_ref[PAD - RIM :, :]


def filtered(rows, taps, rim, pad_ref):
    length, width = rows.shape
    span = taps.shape[0]
    if rim is None:
        rim = jnp.zeros((RIM, width), F32)
    pad_ref[PAD - RIM : PAD, 0:width] = rim
    pad_ref[PAD : PAD + length, 0:width] = rows
    total = rows * taps[span - 1 : span, :]
    for k in range(span - 1):
        back = span - 1 - k
        total = total + pad_ref[PAD - back : PAD - back + length, 0:width] * taps[k : k + 1, :]
    return total


def column(row):
    size = row.shape[1]
    here = lax.broadcasted_iota(jnp.int32, (size, size), 0) == lax.broadcasted_iota(
        jnp.int32, (size, size), 1
    )
    return jnp.sum(jnp.where(here, jnp.broadcast_to(row, (size, size)), 0.0), axis=1, keepdims=True)


def prepare_kernel(
    x_hbm, w_hbm, r_hbm, i_hbm, v_hbm, o_hbm, gate_hbm, xt_hbm, wt_hbm, rt_hbm, ct_hbm, scale_hbm,
    step_hbm, spike_hbm, off_hbm, rate_hbm,
    weighted_ref, writes_ref, reads_ref, inside_ref, conv_ref, open_ref, head_ref,
    xt_ref, wt_ref, rt_ref, ct_ref, scale_ref, dt_ref, rise_ref, remain_ref,
    x_ref, w_ref, r_ref, i_ref, v_ref, o_ref, gate_ref,
    step_ref, spike_ref, off_ref, rate_ref, pad_ref, sems,
):
    width = x_hbm.shape[2]
    narrow = w_hbm.shape[2]
    broad = i_hbm.shape[2]
    copies = fetch(
        (
            (step_hbm.at[0], step_ref),
            (spike_hbm, spike_ref),
            (off_hbm, off_ref),
            (rate_hbm, rate_ref),
            (w_hbm.at[0], w_ref),
            (wt_hbm, wt_ref),
            (r_hbm.at[0], r_ref),
            (rt_hbm, rt_ref),
            (x_hbm.at[0], x_ref),
            (xt_hbm, xt_ref),
            (gate_hbm.at[0], gate_ref),
            (i_hbm.at[0], i_ref),
            (v_hbm.at[0], v_ref),
            (o_hbm.at[0], o_ref),
            (ct_hbm, ct_ref),
            (scale_hbm, scale_ref),
        ),
        sems,
    )
    for copy in copies[:4]:
        copy.wait()
    heads, length = step_ref.shape
    raw = step_ref[...] + column(off_ref[...])
    dt_t = jnp.maximum(raw, 0.0) + jnp.log1p(jnp.exp(-jnp.abs(raw)))
    fall_t = spike_ref[...] - dt_t * column(jnp.exp(rate_ref[...]))
    row = lax.broadcasted_iota(jnp.int32, (length, length), 0)
    col = lax.broadcasted_iota(jnp.int32, (length, length), 1)
    rise_t = jnp.dot(
        fall_t, (row <= col).astype(F32), precision=lax.Precision.HIGHEST, preferred_element_type=F32
    )
    tall = jnp.concatenate([rise_t, dt_t, jnp.zeros((LANES - 2 * heads, length), F32)], axis=0)
    turned_over = jnp.transpose(tall)
    rise = turned_over[:, 0:heads]
    dt = turned_over[:, heads : 2 * heads]
    rise_ref[...] = rise
    dt_ref[...] = dt[0:HEAD, :]
    remain = jnp.exp(jnp.minimum(rise[length - 1 : length, :] - rise, 0.0))
    remain_ref[...] = remain[0:HEAD, :]
    for copy in copies[4:8]:
        copy.wait()
    groups = narrow // STATE
    per_group = width // LANES // groups
    scores = []
    for g in range(groups):
        cols = slice(g * STATE, (g + 1) * STATE)
        write = silu(
            filtered(w_ref[:, cols].astype(F32), wt_ref[:, cols].astype(F32), None, pad_ref)
        ).astype(BF16)
        read = silu(
            filtered(r_ref[:, cols].astype(F32), rt_ref[:, cols].astype(F32), None, pad_ref)
        ).astype(BF16)
        writes_ref[:, cols] = write
        reads_ref[:, cols] = read
        score = lax.dot_general(read, write, (((1,), (1,)), ((), ())), preferred_element_type=F32)
        scores.append(jnp.where(row >= col, score, 0.0))
    for copy in copies[8:10]:
        copy.wait()
    low = lax.broadcasted_iota(jnp.int32, (length, LANES), 1) < HEAD_DIM
    late = lax.broadcasted_iota(jnp.int32, (length, LANES), 0) >= HEAD
    for q in range(width // LANES):
        cols = slice(q * LANES, (q + 1) * LANES)
        x = silu(filtered(x_ref[:, cols].astype(F32), xt_ref[:, cols].astype(F32), None, pad_ref))
        x = x * pair_lanes(dt, q, length)
        weighted_ref[:, cols] = (x * pair_lanes(remain, q, length)).astype(BF16)
        stacked = jnp.concatenate(
            [
                jnp.where(low & late, x, 0.0).astype(BF16),
                jnp.where(late & ~low, x, 0.0).astype(BF16),
            ],
            axis=0,
        )
        both = []
        for h in (2 * q, 2 * q + 1):
            gap = jnp.minimum(rise[:, h : h + 1] - rise_t[h : h + 1, :], 0.0)
            both.append((scores[q // per_group] * jnp.exp(gap)).astype(BF16))
        inside_ref[:, cols] = jnp.dot(
            jnp.concatenate(both, axis=1), stacked, preferred_element_type=F32
        )
    for copy in copies[10:]:
        copy.wait()
    for c in range(0, width, LANES):
        open_ref[:, c : c + LANES] = silu(gate_ref[:, c : c + LANES].astype(F32))
    for c in range(0, broad, LANES):
        cols = slice(c, c + LANES)
        product = i_ref[:, cols].astype(F32) * v_ref[:, cols].astype(F32)
        total = filtered(product, ct_ref[:, cols].astype(F32), None, pad_ref)
        conv_ref[:, cols] = (o_ref[:, cols].astype(F32) * total).astype(BF16)
    at = 0
    for ref in (x_ref, w_ref, r_ref, i_ref, v_ref, o_ref):
        head_ref[:, at : at + ref.shape[1]] = ref[0:HEAD, :]
        at += ref.shape[1]


def state_kernel(
    rim_ref, weighted_ref, writes_ref, reads_in, inside_in, conv_in, head_ref,
    xt_ref, wt_ref, rt_ref, ct_ref, dt_ref, rise_ref, remain_ref,
    pay_ref, reads_ref, inside_ref, conv_ref, pad_ref,
):
    length, width = weighted_ref.shape
    heads = rise_ref.shape[1]
    narrow = writes_ref.shape[1]
    broad = conv_in.shape[1]
    groups = narrow // STATE
    per_group = width // LANES // groups
    sub = lax.broadcasted_iota(jnp.int32, (EXTRA, LANES), 0)
    rise = rise_ref[...]
    total = rise[length - 1 : length, :]
    dt = dt_ref[...]
    remain = remain_ref[...]
    blocks = STATE // 16

    def first(taps_ref, cols, spot):
        return silu(
            filtered(
                head_ref[:, spot].astype(F32),
                taps_ref[:, cols].astype(F32),
                rim_ref[:, spot].astype(F32),
                pad_ref,
            )
        )

    lane = lax.broadcasted_iota(jnp.int32, (length, LANES), 1)
    row = lax.broadcasted_iota(jnp.int32, (length, LANES), 0)
    share = heads // groups
    for g in range(groups):
        cols = slice(g * STATE, (g + 1) * STATE)
        spot = slice(width + g * STATE, width + (g + 1) * STATE)
        first_write = first(wt_ref, cols, spot).astype(BF16)
        write = jnp.concatenate([first_write, writes_ref[HEAD:, cols]], axis=0)
        write_t = jnp.transpose(write.astype(F32)).astype(BF16)
        firsts = []
        for q in range(g * per_group, (g + 1) * per_group):
            pair = slice(q * LANES, (q + 1) * LANES)
            x = first(xt_ref, pair, pair) * pair_lanes(dt, q, HEAD)
            firsts.append(x.astype(BF16))
            x = (x * pair_lanes(remain, q, HEAD)).astype(BF16)
            weighted = jnp.concatenate([x, weighted_ref[HEAD:, pair]], axis=0)
            state = jnp.dot(write_t, weighted, preferred_element_type=F32)
            pay_ref[q * blocks : (q + 1) * blocks, 0:16, :] = state.reshape(blocks, 16, LANES).astype(BF16)
            t = pair_lanes(total, q, 1)
            hi = t.astype(BF16).astype(F32)
            mid = (t - hi).astype(BF16).astype(F32)
            lo = t - hi - mid
            terms = jnp.where(sub == 0, hi, jnp.where(sub == 1, mid, jnp.where(sub == 2, lo, 0.0))).astype(BF16)
            pay_ref[q * blocks : (q + 1) * blocks, 16 : 16 + EXTRA, :] = jnp.broadcast_to(terms[None], (blocks, EXTRA, LANES))
        spot = slice(width + narrow + g * STATE, width + narrow + (g + 1) * STATE)
        read = jnp.concatenate([first(rt_ref, cols, spot).astype(BF16), reads_in[HEAD:, cols]], axis=0)
        reads_ref[:, cols] = read
        scores = lax.dot_general(
            read, jnp.concatenate([first_write] * share, axis=0), (((1,), (1,)), ((), ())),
            preferred_element_type=F32,
        )
        spread = (
            lax.broadcasted_iota(jnp.int32, (heads, LANES), 0)
            == g * share + lax.broadcasted_iota(jnp.int32, (heads, LANES), 1) // HEAD
        ).astype(F32)
        rises = jnp.dot(rise, spread, precision=lax.Precision.HIGHEST, preferred_element_type=F32)
        here = (row == lane % HEAD)[0:HEAD]
        start = jnp.sum(jnp.where(here, rises[0:HEAD], 0.0), axis=0, keepdims=True)
        kept = jnp.where(
            lane % HEAD <= row, scores * jnp.exp(jnp.minimum(rises - start, 0.0)), 0.0
        ).astype(BF16)
        span = per_group * LANES
        tiled = jnp.concatenate([jnp.concatenate(firsts, axis=1)] * share, axis=0)
        own = (
            lax.broadcasted_iota(jnp.int32, (LANES, span), 0) // HEAD
            == lax.broadcasted_iota(jnp.int32, (LANES, span), 1) // HEAD_DIM
        )
        tiled = jnp.where(own, tiled, jnp.zeros_like(tiled))
        wide = slice(g * span, (g + 1) * span)
        inside_ref[:, wide] = inside_in[:, wide] + jnp.dot(kept, tiled, preferred_element_type=F32)
    base = width + 2 * narrow
    for c in range(0, broad, LANES):
        cols = slice(c, c + LANES)
        i = slice(base + c, base + c + LANES)
        v = slice(base + broad + c, base + broad + c + LANES)
        o = slice(base + 2 * broad + c, base + 2 * broad + c + LANES)
        product = head_ref[:, i].astype(F32) * head_ref[:, v].astype(F32)
        rim = rim_ref[:, i].astype(F32) * rim_ref[:, v].astype(F32)
        value = filtered(product, ct_ref[:, cols].astype(F32), rim, pad_ref)
        conv_ref[0:HEAD, cols] = (head_ref[:, o].astype(F32) * value).astype(BF16)
        conv_ref[HEAD:, cols] = conv_in[HEAD:, cols]


def turned(members, first):
    return [[(k + first) % members for k in range(members)]]


def scan_kernel(in_ref, out_ref):
    members = in_ref.shape[0]
    carry = jnp.zeros((16, LANES), F32)
    for j in range(members):
        at = (j - FIRST_OUT) % members
        out_ref[(j - FIRST_BACK) % members] = carry.astype(BF16)
        if j + 1 < members:
            t = in_ref[at, 16 : 16 + EXTRA, :].astype(F32)
            decay = jnp.exp(t[0:1, :] + t[1:2, :] + t[2:3, :])
            carry = carry * decay + in_ref[at, 0:16, :].astype(F32)


def gate_kernel(p_ref, reads_ref, rise_ref, inside_ref, open_ref, scale_ref, conv_ref, out_ref):
    length, width = inside_ref.shape
    groups = reads_ref.shape[1] // STATE
    per_group = width // LANES // groups
    kept = jnp.exp(rise_ref[...])
    blocks = STATE // 16
    copies = out_ref.shape[0]
    for g in range(groups):
        read = reads_ref[:, g * STATE : (g + 1) * STATE]
        squares = jnp.zeros((length, LANES), F32)
        gated = []
        for q in range(g * per_group, (g + 1) * per_group):
            cols = slice(q * LANES, (q + 1) * LANES)
            spots = [(q * blocks + k + FIRST_OUT - FIRST_BACK) % p_ref.shape[0] for k in range(blocks)]
            before = jnp.concatenate([p_ref[spot] for spot in spots], axis=0)
            carried = jnp.dot(read, before, preferred_element_type=F32)
            y = inside_ref[:, cols] + carried * pair_lanes(kept, q, length)
            y = y * open_ref[:, cols]
            squares = squares + y * y
            gated.append(y)
        mean = jnp.sum(squares, axis=1, keepdims=True) * (1.0 / (per_group * LANES))
        inverse = lax.rsqrt(mean + EPS)
        for k, q in enumerate(range(g * per_group, (g + 1) * per_group)):
            cols = slice(q * LANES, (q + 1) * LANES)
            value = (gated[k] * inverse * scale_ref[:, cols]).astype(BF16)
            for c in range(copies):
                out_ref[c, :, cols] = value
    for c in range(copies):
        out_ref[c, :, width:] = conv_ref[...]


def project_kernel(half_ref, a_ref, s_ref, c_ref, out_ref):
    seqs, length, depth = a_ref.shape
    width = s_ref.shape[0]
    start = half_ref[0]
    for k in range(seqs // 2):
        rows = a_ref[start + k]
        out_ref[k] = (
            jnp.dot(rows[:, :width], s_ref[...], preferred_element_type=F32)
            + jnp.dot(rows[:, width:], c_ref[...], preferred_element_type=F32)
        ).astype(out_ref.dtype)


def project(half, rows, s, c, dtype):
    seqs, length, _ = rows.shape
    out = jax.ShapeDtypeStruct((seqs // 2, length, s.shape[1]), dtype)
    ins = (half, rows, s, c)
    return pl.pallas_call(
        project_kernel,
        grid=(1,),
        in_specs=[pl.BlockSpec(memory_space=pltpu.SMEM)] + [whole(a.shape) for a in ins[1:]],
        out_specs=whole(out.shape),
        out_shape=out,
        compiler_params=pltpu.CompilerParams(vmem_limit_bytes=24 * 1024 * 1024),
        cost_estimate=pl.CostEstimate(
            flops=400_000_000, bytes_accessed=2_000_000, transcendentals=0
        ),
    )(*ins)


def merge_kernel(kept_ref, got_ref, out_ref):
    out_ref[...] = (kept_ref[...] + got_ref[...].astype(F32)).astype(BF16)


def per_device(
    output_gate_logits,
    head_input_rows,
    group_state_writes,
    group_state_reads,
    step_logits,
    head_step_offset,
    head_decay_logrates,
    decay_extra_spikes,
    head_input_taps,
    state_input_taps,
    readout_filter_taps,
    grouped_norm_scale,
    convolution_outer_gate,
    convolution_inner_gate,
    convolution_value_rows,
    gated_filter_taps,
    state_output_rows,
    convolution_output_rows,
):
    sds = jax.ShapeDtypeStruct
    _, length, width = head_input_rows.shape
    heads = step_logits.shape[2]
    narrow = group_state_writes.shape[2]
    wide = convolution_inner_gate.shape[2]
    members = lax.axis_size("sp")
    copies = lax.axis_size("fs")
    ends = (
        head_input_rows,
        group_state_writes,
        group_state_reads,
        convolution_inner_gate,
        convolution_value_rows,
    )
    all_width = sum(a.shape[2] for a in ends)
    rims = call(
        rims_kernel, [sds((RIM, all_width), BF16)], ends, 5, [vmem((PAD, all_width), BF16), sems(5)], 1000
    )[0]
    before = lax.ppermute(rims, "sp", [(k, k + 1) for k in range(members - 1)])
    ins = (
        *ends, convolution_outer_gate, output_gate_logits,
        head_input_taps, state_input_taps, readout_filter_taps, gated_filter_taps,
        grouped_norm_scale[None], jnp.swapaxes(step_logits, 1, 2), decay_extra_spikes.T,
        head_step_offset[None], head_decay_logrates[None],
    )
    tall = sds((length, width), BF16)
    slim = sds((length, narrow), BF16)
    side = sds((length, wide), BF16)
    full = sds((length, width), F32)
    outs = [
        tall, slim, slim, full, side, full, sds((HEAD, all_width + wide), BF16),
        sds(head_input_taps.shape, BF16), sds(state_input_taps.shape, BF16),
        sds(readout_filter_taps.shape, BF16), sds(gated_filter_taps.shape, BF16),
        sds((1, width), F32), sds((HEAD, heads), F32), sds((length, heads), F32), sds((HEAD, heads), F32),
    ]
    pad = vmem((PAD + length, LANES))
    scratch = [vmem(a.shape[1:], BF16) for a in ins[:7]] + [
        vmem((heads, length)),
        vmem((heads, length)),
        vmem((1, heads)),
        vmem((1, heads)),
        pad,
        sems(16),
    ]
    (
        weighted, writes, reads, inside, conv, opened, head, xt, wt, rt, ct, scale, dt, rise, remain,
    ) = call(prepare_kernel, outs, ins, 16, scratch)
    ins = (before, weighted, writes, reads, inside, conv, head, xt, wt, rt, ct, dt, rise, remain)
    outs = [sds((members, 16 + EXTRA, LANES), BF16), slim, full, side]
    payload, reads, inside, conv = call(state_kernel, outs, ins, 0, [pad])
    core = lax.axis_index("tp")
    seqs = copies
    mine = (core * (seqs // 2)).astype(jnp.int32)[None]
    theirs = ((1 - core) * (seqs // 2)).astype(jnp.int32)[None]
    payload, mine, theirs = lax.optimization_barrier((payload, mine, theirs))
    gathered = lax.all_to_all(
        payload, "sp", 0, 0, axis_index_groups=turned(members, FIRST_OUT), tiled=True
    )
    prefixes = call(scan_kernel, [sds((members, 16, LANES), BF16)], (gathered,))[0]
    incoming = lax.all_to_all(prefixes, "sp", 0, 0, axis_index_groups=turned(members, FIRST_BACK), tiled=True)
    ins = (incoming, reads, rise, inside, opened, scale, conv)
    joined = call(gate_kernel, [sds((copies, length, width + wide), BF16)], ins)[0]
    rows = lax.all_to_all(joined, "fs", 0, 0, tiled=True)
    sent = project(theirs, rows, state_output_rows, convolution_output_rows, BF16)
    got = lax.ppermute(sent, "tp", [(0, 1), (1, 0)])
    kept = project(mine, rows, state_output_rows, convolution_output_rows, F32)
    return call(merge_kernel, [sds(got.shape, BF16)], (kept, got))[0]


def solution(mesh):
    return jax.shard_map(
        per_device,
        mesh=mesh,
        in_specs=(
            P("fs", "sp", "tp"),
            P("fs", "sp", "tp"),
            P("fs", "sp", "tp"),
            P("fs", "sp", "tp"),
            P("fs", "sp", "tp"),
            P("tp"),
            P("tp"),
            P("sp", "tp"),
            P(None, "tp"),
            P(None, "tp"),
            P(None, "tp"),
            P("tp"),
            P("fs", "sp", "tp"),
            P("fs", "sp", "tp"),
            P("fs", "sp", "tp"),
            P(None, "tp"),
            P("tp", "fs"),
            P("tp", "fs"),
        ),
        out_specs=P("tp", "sp", "fs"),
        check_vma=False,
    )
```

```python
import functools

import jax
import jax.numpy as jnp
from jax import lax
from jax.experimental import pallas as pl
from jax.experimental.pallas import tpu as pltpu
from jax.sharding import PartitionSpec as P


EPS = 1e-06
F32 = jnp.float32
BF16 = jnp.bfloat16
STATE = 128
LANES = 128
HEAD_DIM = 64
EXTRA = 8
PAD = 8
RIM = 4
HEAD = 16
FIRST_OUT = 52
FIRST_BACK = 52


def whole(shape):
    return pl.BlockSpec(shape, lambda *_: (0,) * len(shape))


HBM = pl.BlockSpec(memory_space=pltpu.HBM)


def call(kernel, outs, ins, far=0, scratch=(), flops=50_000_000):
    ins = [pltpu.with_memory_space_constraint(a, pltpu.HBM) for a in ins[:far]] + list(ins[far:])
    return pl.pallas_call(
        kernel,
        grid=(1,),
        in_specs=[HBM] * far + [whole(a.shape) for a in ins[far:]],
        out_specs=[whole(o.shape) for o in outs],
        out_shape=outs,
        scratch_shapes=scratch,
        compiler_params=pltpu.CompilerParams(vmem_limit_bytes=24 * 1024 * 1024),
        cost_estimate=pl.CostEstimate(flops=flops, bytes_accessed=2_000_000, transcendentals=0),
    )(*ins)


def vmem(shape, dtype=F32):
    return pltpu.VMEM(shape, dtype)


def sems(count):
    return pltpu.SemaphoreType.DMA((count,))


def silu(v):
    return v / (1.0 + jnp.exp(-v))


def pair_lanes(cols, q, rows):
    low = lax.broadcasted_iota(jnp.int32, (rows, LANES), 1) < HEAD_DIM
    first = jnp.broadcast_to(cols[:, 2 * q : 2 * q + 1], (rows, LANES))
    second = jnp.broadcast_to(cols[:, 2 * q + 1 : 2 * q + 2], (rows, LANES))
    return jnp.where(low, first, second)


def fetch(pairs, sems):
    copies = [pltpu.make_async_copy(src, dst, sems.at[k]) for k, (src, dst) in enumerate(pairs)]
    for copy in copies:
        copy.start()
    return copies


def filtered(rows, taps, rim, pad_ref):
    length, width = rows.shape
    span = taps.shape[0]
    if rim is None:
        rim = jnp.zeros((RIM, width), F32)
    pad_ref[PAD - RIM : PAD, 0:width] = rim
    pad_ref[PAD : PAD + length, 0:width] = rows
    total = rows * taps[span - 1 : span, :]
    for k in range(span - 1):
        back = span - 1 - k
        total = total + pad_ref[PAD - back : PAD - back + length, 0:width] * taps[k : k + 1, :]
    return total


def column(row):
    size = row.shape[1]
    here = lax.broadcasted_iota(jnp.int32, (size, size), 0) == lax.broadcasted_iota(
        jnp.int32, (size, size), 1
    )
    return jnp.sum(jnp.where(here, jnp.broadcast_to(row, (size, size)), 0.0), axis=1, keepdims=True)


def prepare_kernel(
    x_hbm, w_hbm, r_hbm, i_hbm, v_hbm, o_hbm, gate_hbm, xt_hbm, wt_hbm, rt_hbm, ct_hbm, scale_hbm,
    step_hbm, spike_hbm, off_hbm, rate_hbm, s_hbm, c_hbm,
    weighted_ref, writes_ref, reads_ref, inside_ref, conv_ref, open_ref, head_ref,
    xt_ref, wt_ref, rt_ref, ct_ref, scale_ref, dt_ref, rise_ref, remain_ref, both_ref, rim_ref,
    x_ref, w_ref, r_ref, i_ref, v_ref, o_ref, gate_ref,
    step_ref, spike_ref, off_ref, rate_ref, pad_ref, sems,
):
    width = x_hbm.shape[2]
    narrow = w_hbm.shape[2]
    broad = i_hbm.shape[2]
    copies = fetch(
        (
            (step_hbm.at[0], step_ref),
            (spike_hbm, spike_ref),
            (off_hbm, off_ref),
            (rate_hbm, rate_ref),
            (w_hbm.at[0], w_ref),
            (wt_hbm, wt_ref),
            (r_hbm.at[0], r_ref),
            (rt_hbm, rt_ref),
            (x_hbm.at[0], x_ref),
            (xt_hbm, xt_ref),
            (gate_hbm.at[0], gate_ref),
            (i_hbm.at[0], i_ref),
            (v_hbm.at[0], v_ref),
            (o_hbm.at[0], o_ref),
            (ct_hbm, ct_ref),
            (scale_hbm, scale_ref),
            (s_hbm, both_ref.at[pl.ds(0, s_hbm.shape[0])]),
            (c_hbm, both_ref.at[pl.ds(s_hbm.shape[0], c_hbm.shape[0])]),
        ),
        sems,
    )
    for copy in copies[:4]:
        copy.wait()
    heads, length = step_ref.shape
    raw = step_ref[...] + column(off_ref[...])
    dt_t = jnp.maximum(raw, 0.0) + jnp.log1p(jnp.exp(-jnp.abs(raw)))
    fall_t = spike_ref[...] - dt_t * column(jnp.exp(rate_ref[...]))
    row = lax.broadcasted_iota(jnp.int32, (length, length), 0)
    col = lax.broadcasted_iota(jnp.int32, (length, length), 1)
    rise_t = jnp.dot(
        fall_t, (row <= col).astype(F32), precision=lax.Precision.HIGHEST, preferred_element_type=F32
    )
    tall = jnp.concatenate([rise_t, dt_t, jnp.zeros((LANES - 2 * heads, length), F32)], axis=0)
    turned_over = jnp.transpose(tall)
    rise = turned_over[:, 0:heads]
    dt = turned_over[:, heads : 2 * heads]
    rise_ref[...] = rise
    dt_ref[...] = dt[0:HEAD, :]
    remain = jnp.exp(jnp.minimum(rise[length - 1 : length, :] - rise, 0.0))
    remain_ref[...] = remain[0:HEAD, :]
    for copy in copies[4:8]:
        copy.wait()
    groups = narrow // STATE
    per_group = width // LANES // groups
    scores = []
    for g in range(groups):
        cols = slice(g * STATE, (g + 1) * STATE)
        write = silu(
            filtered(w_ref[:, cols].astype(F32), wt_ref[:, cols].astype(F32), None, pad_ref)
        ).astype(BF16)
        read = silu(
            filtered(r_ref[:, cols].astype(F32), rt_ref[:, cols].astype(F32), None, pad_ref)
        ).astype(BF16)
        writes_ref[:, cols] = write
        reads_ref[:, cols] = read
        score = lax.dot_general(read, write, (((1,), (1,)), ((), ())), preferred_element_type=F32)
        scores.append(jnp.where(row >= col, score, 0.0))
    for copy in copies[8:10]:
        copy.wait()
    low = lax.broadcasted_iota(jnp.int32, (length, LANES), 1) < HEAD_DIM
    late = lax.broadcasted_iota(jnp.int32, (length, LANES), 0) >= HEAD
    for q in range(width // LANES):
        cols = slice(q * LANES, (q + 1) * LANES)
        x = silu(filtered(x_ref[:, cols].astype(F32), xt_ref[:, cols].astype(F32), None, pad_ref))
        x = x * pair_lanes(dt, q, length)
        weighted_ref[:, cols] = (x * pair_lanes(remain, q, length)).astype(BF16)
        stacked = jnp.concatenate(
            [
                jnp.where(low & late, x, 0.0).astype(BF16),
                jnp.where(late & ~low, x, 0.0).astype(BF16),
            ],
            axis=0,
        )
        both = []
        for h in (2 * q, 2 * q + 1):
            gap = jnp.minimum(rise[:, h : h + 1] - rise_t[h : h + 1, :], 0.0)
            both.append((scores[q // per_group] * jnp.exp(gap)).astype(BF16))
        inside_ref[:, cols] = jnp.dot(
            jnp.concatenate(both, axis=1), stacked, preferred_element_type=F32
        )
    for copy in copies[10:]:
        copy.wait()
    for c in range(0, width, LANES):
        open_ref[:, c : c + LANES] = silu(gate_ref[:, c : c + LANES].astype(F32))
    for c in range(0, broad, LANES):
        cols = slice(c, c + LANES)
        product = i_ref[:, cols].astype(F32) * v_ref[:, cols].astype(F32)
        total = filtered(product, ct_ref[:, cols].astype(F32), None, pad_ref)
        conv_ref[:, cols] = (o_ref[:, cols].astype(F32) * total).astype(BF16)
    at = 0
    for ref in (x_ref, w_ref, r_ref, i_ref, v_ref, o_ref):
        head_ref[:, at : at + ref.shape[1]] = ref[0:HEAD, :]
        if ref is not o_ref:
            rim_ref[:, at : at + ref.shape[1]] = ref[length - RIM : length, :]
        at += ref.shape[1]


def state_kernel(
    rim_ref, weighted_ref, writes_ref, reads_in, inside_in, conv_in, head_ref,
    xt_ref, wt_ref, rt_ref, ct_ref, dt_ref, rise_ref, remain_ref,
    pay_ref, reads_ref, inside_ref, conv_ref, pad_ref,
):
    length, width = weighted_ref.shape
    heads = rise_ref.shape[1]
    narrow = writes_ref.shape[1]
    broad = conv_in.shape[1]
    groups = narrow // STATE
    per_group = width // LANES // groups
    sub = lax.broadcasted_iota(jnp.int32, (EXTRA, LANES), 0)
    rise = rise_ref[...]
    total = rise[length - 1 : length, :]
    dt = dt_ref[...]
    remain = remain_ref[...]
    blocks = STATE // 16

    def first(taps_ref, cols, spot):
        return silu(
            filtered(
                head_ref[:, spot].astype(F32),
                taps_ref[:, cols].astype(F32),
                rim_ref[:, spot].astype(F32),
                pad_ref,
            )
        )

    lane = lax.broadcasted_iota(jnp.int32, (length, LANES), 1)
    row = lax.broadcasted_iota(jnp.int32, (length, LANES), 0)
    share = heads // groups
    for g in range(groups):
        cols = slice(g * STATE, (g + 1) * STATE)
        spot = slice(width + g * STATE, width + (g + 1) * STATE)
        first_write = first(wt_ref, cols, spot).astype(BF16)
        write = jnp.concatenate([first_write, writes_ref[HEAD:, cols]], axis=0)
        write_t = jnp.transpose(write.astype(F32)).astype(BF16)
        firsts = []
        for q in range(g * per_group, (g + 1) * per_group):
            pair = slice(q * LANES, (q + 1) * LANES)
            x = first(xt_ref, pair, pair) * pair_lanes(dt, q, HEAD)
            firsts.append(x.astype(BF16))
            x = (x * pair_lanes(remain, q, HEAD)).astype(BF16)
            weighted = jnp.concatenate([x, weighted_ref[HEAD:, pair]], axis=0)
            state = jnp.dot(write_t, weighted, preferred_element_type=F32)
            pay_ref[q * blocks : (q + 1) * blocks, 0:16, :] = state.reshape(blocks, 16, LANES).astype(BF16)
            t = pair_lanes(total, q, 1)
            hi = t.astype(BF16).astype(F32)
            mid = (t - hi).astype(BF16).astype(F32)
            lo = t - hi - mid
            terms = jnp.where(sub == 0, hi, jnp.where(sub == 1, mid, jnp.where(sub == 2, lo, 0.0))).astype(BF16)
            pay_ref[q * blocks : (q + 1) * blocks, 16 : 16 + EXTRA, :] = jnp.broadcast_to(terms[None], (blocks, EXTRA, LANES))
        spot = slice(width + narrow + g * STATE, width + narrow + (g + 1) * STATE)
        read = jnp.concatenate([first(rt_ref, cols, spot).astype(BF16), reads_in[HEAD:, cols]], axis=0)
        reads_ref[:, cols] = read
        scores = lax.dot_general(
            read, jnp.concatenate([first_write] * share, axis=0), (((1,), (1,)), ((), ())),
            preferred_element_type=F32,
        )
        spread = (
            lax.broadcasted_iota(jnp.int32, (heads, LANES), 0)
            == g * share + lax.broadcasted_iota(jnp.int32, (heads, LANES), 1) // HEAD
        ).astype(F32)
        rises = jnp.dot(rise, spread, precision=lax.Precision.HIGHEST, preferred_element_type=F32)
        here = (row == lane % HEAD)[0:HEAD]
        start = jnp.sum(jnp.where(here, rises[0:HEAD], 0.0), axis=0, keepdims=True)
        kept = jnp.where(
            lane % HEAD <= row, scores * jnp.exp(jnp.minimum(rises - start, 0.0)), 0.0
        ).astype(BF16)
        span = per_group * LANES
        tiled = jnp.concatenate([jnp.concatenate(firsts, axis=1)] * share, axis=0)
        own = (
            lax.broadcasted_iota(jnp.int32, (LANES, span), 0) // HEAD
            == lax.broadcasted_iota(jnp.int32, (LANES, span), 1) // HEAD_DIM
        )
        tiled = jnp.where(own, tiled, jnp.zeros_like(tiled))
        wide = slice(g * span, (g + 1) * span)
        inside_ref[:, wide] = inside_in[:, wide] + jnp.dot(kept, tiled, preferred_element_type=F32)
    base = width + 2 * narrow
    for c in range(0, broad, LANES):
        cols = slice(c, c + LANES)
        i = slice(base + c, base + c + LANES)
        v = slice(base + broad + c, base + broad + c + LANES)
        o = slice(base + 2 * broad + c, base + 2 * broad + c + LANES)
        product = head_ref[:, i].astype(F32) * head_ref[:, v].astype(F32)
        rim = rim_ref[:, i].astype(F32) * rim_ref[:, v].astype(F32)
        value = filtered(product, ct_ref[:, cols].astype(F32), rim, pad_ref)
        conv_ref[0:HEAD, cols] = (head_ref[:, o].astype(F32) * value).astype(BF16)
        conv_ref[HEAD:, cols] = conv_in[HEAD:, cols]


def turned(members, first):
    return [[(k + first) % members for k in range(members)]]


def scan_kernel(in_ref, out_ref):
    members = in_ref.shape[0]
    carry = jnp.zeros((16, LANES), F32)
    for j in range(members):
        at = (j - FIRST_OUT) % members
        out_ref[(j - FIRST_BACK) % members] = carry.astype(BF16)
        if j + 1 < members:
            t = in_ref[at, 16 : 16 + EXTRA, :].astype(F32)
            decay = jnp.exp(t[0:1, :] + t[1:2, :] + t[2:3, :])
            carry = carry * decay + in_ref[at, 0:16, :].astype(F32)


def gate_kernel(p_ref, reads_ref, rise_ref, inside_ref, open_ref, scale_ref, conv_ref, out_ref):
    length, width = inside_ref.shape
    groups = reads_ref.shape[1] // STATE
    per_group = width // LANES // groups
    kept = jnp.exp(rise_ref[...])
    blocks = STATE // 16
    for g in range(groups):
        read = reads_ref[:, g * STATE : (g + 1) * STATE]
        squares = jnp.zeros((length, LANES), F32)
        gated = []
        for q in range(g * per_group, (g + 1) * per_group):
            cols = slice(q * LANES, (q + 1) * LANES)
            spots = [(q * blocks + k + FIRST_OUT - FIRST_BACK) % p_ref.shape[0] for k in range(blocks)]
            before = jnp.concatenate([p_ref[spot] for spot in spots], axis=0)
            carried = jnp.dot(read, before, preferred_element_type=F32)
            y = inside_ref[:, cols] + carried * pair_lanes(kept, q, length)
            y = y * open_ref[:, cols]
            squares = squares + y * y
            gated.append(y)
        mean = jnp.sum(squares, axis=1, keepdims=True) * (1.0 / (per_group * LANES))
        inverse = lax.rsqrt(mean + EPS)
        for k, q in enumerate(range(g * per_group, (g + 1) * per_group)):
            cols = slice(q * LANES, (q + 1) * LANES)
            value = (gated[k] * inverse * scale_ref[:, cols]).astype(BF16)
            out_ref[:, cols] = value
    out_ref[:, width:] = conv_ref[...]


def far_kernel(a_ref, w_ref, out_ref):
    out_ref[...] = jnp.dot(a_ref[...], w_ref[...], preferred_element_type=F32).astype(BF16)


def part_kernel(kept, early, first_ref, second_ref, w_ref, out_ref):
    core = lax.axis_index("tp")
    chip = lax.axis_index("fs")
    odd = lax.rem(chip, 2)
    seq = 2 * (core if kept else 1 - core) + (odd if early else 1 - odd)
    away = lax.rem(seq - chip + 4, 4)

    @pl.when(away < 2)
    def _():
        out_ref[...] = jnp.dot(first_ref[...], w_ref[...], preferred_element_type=F32).astype(out_ref.dtype)

    @pl.when(away >= 2)
    def _():
        if early:
            out_ref[...] = second_ref[...].astype(out_ref.dtype)
        else:
            out_ref[...] = jnp.dot(second_ref[...], w_ref[...], preferred_element_type=F32).astype(out_ref.dtype)


def part(kept, early, first, second, rows):
    out = jax.ShapeDtypeStruct((first.shape[0], rows.shape[1]), F32 if kept else BF16)
    return call(functools.partial(part_kernel, kept, early), [out], (first, second, rows))[0]


def merge_kernel(early_ref, early_got_ref, late_ref, late_got_ref, out_ref):
    odd = lax.rem(lax.axis_index("fs"), 2)
    out_ref[odd] = (early_ref[...] + early_got_ref[...].astype(F32)).astype(BF16)
    out_ref[1 - odd] = (late_ref[...] + late_got_ref[...].astype(F32)).astype(BF16)


def per_device(
    output_gate_logits,
    head_input_rows,
    group_state_writes,
    group_state_reads,
    step_logits,
    head_step_offset,
    head_decay_logrates,
    decay_extra_spikes,
    head_input_taps,
    state_input_taps,
    readout_filter_taps,
    grouped_norm_scale,
    convolution_outer_gate,
    convolution_inner_gate,
    convolution_value_rows,
    gated_filter_taps,
    state_output_rows,
    convolution_output_rows,
):
    sds = jax.ShapeDtypeStruct
    _, length, width = head_input_rows.shape
    heads = step_logits.shape[2]
    narrow = group_state_writes.shape[2]
    wide = convolution_inner_gate.shape[2]
    members = lax.axis_size("sp")
    copies = lax.axis_size("fs")
    ends = (
        head_input_rows,
        group_state_writes,
        group_state_reads,
        convolution_inner_gate,
        convolution_value_rows,
    )
    all_width = sum(a.shape[2] for a in ends)
    ins = (
        *ends, convolution_outer_gate, output_gate_logits,
        head_input_taps, state_input_taps, readout_filter_taps, gated_filter_taps,
        grouped_norm_scale[None], jnp.swapaxes(step_logits, 1, 2), decay_extra_spikes.T,
        head_step_offset[None], head_decay_logrates[None], state_output_rows, convolution_output_rows,
    )
    tall = sds((length, width), BF16)
    slim = sds((length, narrow), BF16)
    side = sds((length, wide), BF16)
    full = sds((length, width), F32)
    outs = [
        tall, slim, slim, full, side, full, sds((HEAD, all_width + wide), BF16),
        sds(head_input_taps.shape, BF16), sds(state_input_taps.shape, BF16),
        sds(readout_filter_taps.shape, BF16), sds(gated_filter_taps.shape, BF16),
        sds((1, width), F32), sds((HEAD, heads), F32), sds((length, heads), F32), sds((HEAD, heads), F32),
        sds((width + wide, state_output_rows.shape[1]), BF16), sds((RIM, all_width), BF16),
    ]
    pad = vmem((PAD + length, LANES))
    scratch = [vmem(a.shape[1:], BF16) for a in ins[:7]] + [
        vmem((heads, length)),
        vmem((heads, length)),
        vmem((1, heads)),
        vmem((1, heads)),
        pad,
        sems(18),
    ]
    (
        weighted, writes, reads, inside, conv, opened, head, xt, wt, rt, ct, scale, dt, rise, remain,
        rows_own, rims,
    ) = call(prepare_kernel, outs, ins, 18, scratch)
    before = lax.ppermute(rims, "sp", [(k, k + 1) for k in range(members - 1)])
    ins = (before, weighted, writes, reads, inside, conv, head, xt, wt, rt, ct, dt, rise, remain)
    outs = [sds((members, 16 + EXTRA, LANES), BF16), slim, full, side]
    payload, reads, inside, conv = call(state_kernel, outs, ins, 0, [pad])
    seqs = copies

    def moved(value, away):
        return lax.ppermute(value, "fs", [(k, (k + away) % seqs) for k in range(seqs)])

    rows_far = moved(rows_own, 2)
    gathered = lax.all_to_all(
        payload, "sp", 0, 0, axis_index_groups=turned(members, FIRST_OUT), tiled=True
    )
    prefixes = call(scan_kernel, [sds((members, 16, LANES), BF16)], (gathered,))[0]
    incoming = lax.all_to_all(prefixes, "sp", 0, 0, axis_index_groups=turned(members, FIRST_BACK), tiled=True)
    ins = (incoming, reads, rise, inside, opened, scale, conv)
    own = call(gate_kernel, [sds((length, width + wide), BF16)], ins)[0]
    last = moved(own, 1)
    following = moved(own, -1)
    partial = call(far_kernel, [sds((length, rows_own.shape[1]), BF16)], (own, rows_far))[0]
    far = moved(partial, 2)
    swap = [(0, 1), (1, 0)]
    sent = part(False, True, own, far, rows_own)
    early_got = lax.ppermute(sent, "tp", swap)
    early = part(True, True, own, far, rows_own)
    sent = part(False, False, following, last, rows_own)
    late_got = lax.ppermute(sent, "tp", swap)
    late = part(True, False, following, last, rows_own)
    out = sds((2, length, rows_own.shape[1]), BF16)
    return call(merge_kernel, [out], (early, early_got, late, late_got))[0]


def solution(mesh):
    return jax.shard_map(
        per_device,
        mesh=mesh,
        in_specs=(
            P("fs", "sp", "tp"),
            P("fs", "sp", "tp"),
            P("fs", "sp", "tp"),
            P("fs", "sp", "tp"),
            P("fs", "sp", "tp"),
            P("tp"),
            P("tp"),
            P("sp", "tp"),
            P(None, "tp"),
            P(None, "tp"),
            P(None, "tp"),
            P("tp"),
            P("fs", "sp", "tp"),
            P("fs", "sp", "tp"),
            P("fs", "sp", "tp"),
            P(None, "tp"),
            P("tp", "fs"),
            P("tp", "fs"),
        ),
        out_specs=P("tp", "sp", "fs"),
        check_vma=False,
    )
```

```python
import functools

import jax
import jax.numpy as jnp
from jax import lax
from jax.experimental import pallas as pl
from jax.experimental.pallas import tpu as pltpu
from jax.sharding import PartitionSpec as P


EPS = 1e-06
F32 = jnp.float32
BF16 = jnp.bfloat16
STATE = 128
LANES = 128
HEAD_DIM = 64
EXTRA = 8
PAD = 8
RIM = 4
HEAD = 16
FIRST_OUT = 52
FIRST_BACK = 60


def whole(shape):
    return pl.BlockSpec(shape, lambda *_: (0,) * len(shape))


HBM = pl.BlockSpec(memory_space=pltpu.HBM)


def call(kernel, outs, ins, far=0, scratch=(), flops=50_000_000):
    ins = [pltpu.with_memory_space_constraint(a, pltpu.HBM) for a in ins[:far]] + list(ins[far:])
    return pl.pallas_call(
        kernel,
        grid=(1,),
        in_specs=[HBM] * far + [whole(a.shape) for a in ins[far:]],
        out_specs=[whole(o.shape) for o in outs],
        out_shape=outs,
        scratch_shapes=scratch,
        compiler_params=pltpu.CompilerParams(vmem_limit_bytes=24 * 1024 * 1024),
        cost_estimate=pl.CostEstimate(flops=flops, bytes_accessed=2_000_000, transcendentals=0),
    )(*ins)


def vmem(shape, dtype=F32):
    return pltpu.VMEM(shape, dtype)


def sems(count):
    return pltpu.SemaphoreType.DMA((count,))


def silu(v):
    return v / (1.0 + jnp.exp(-v))


def pair_lanes(cols, q, rows):
    low = lax.broadcasted_iota(jnp.int32, (rows, LANES), 1) < HEAD_DIM
    first = jnp.broadcast_to(cols[:, 2 * q : 2 * q + 1], (rows, LANES))
    second = jnp.broadcast_to(cols[:, 2 * q + 1 : 2 * q + 2], (rows, LANES))
    return jnp.where(low, first, second)


def three(cols):
    high = cols.astype(BF16)
    rest = cols - high.astype(F32)
    middle = rest.astype(BF16)
    return jnp.concatenate([high, middle, (rest - middle.astype(F32)).astype(BF16)], axis=1)


def spread(parts, first, lanes, width):
    heads = parts.shape[1] // 3
    shape = (parts.shape[1], width)
    wanted = first + (lax.broadcasted_iota(jnp.int32, shape, 1) >> (lanes.bit_length() - 1))
    chosen = (lax.broadcasted_iota(jnp.int32, shape, 0) & (heads - 1)) == wanted
    return jnp.dot(parts, chosen.astype(BF16), preferred_element_type=F32)


def fetch(pairs, sems):
    copies = [pltpu.make_async_copy(src, dst, sems.at[k]) for k, (src, dst) in enumerate(pairs)]
    for copy in copies:
        copy.start()
    return copies


def filtered(rows, taps, rim, pad_ref):
    length, width = rows.shape
    span = taps.shape[0]
    if rim is None:
        rim = jnp.zeros((RIM, width), F32)
    pad_ref[PAD - RIM : PAD, 0:width] = rim
    pad_ref[PAD : PAD + length, 0:width] = rows
    total = rows * taps[span - 1 : span, :]
    for k in range(span - 1):
        back = span - 1 - k
        total = total + pad_ref[PAD - back : PAD - back + length, 0:width] * taps[k : k + 1, :]
    return total


def column(row):
    size = row.shape[1]
    here = lax.broadcasted_iota(jnp.int32, (size, size), 0) == lax.broadcasted_iota(
        jnp.int32, (size, size), 1
    )
    return jnp.sum(jnp.where(here, jnp.broadcast_to(row, (size, size)), 0.0), axis=1, keepdims=True)


def prepare_kernel(
    x_hbm, w_hbm, r_hbm, i_hbm, v_hbm, o_hbm, gate_hbm, xt_hbm, wt_hbm, rt_hbm, ct_hbm, scale_hbm,
    step_hbm, spike_hbm, off_hbm, rate_hbm, s_hbm, c_hbm,
    weighted_ref, writes_ref, reads_ref, inside_ref, conv_ref, open_ref, head_ref,
    xt_ref, wt_ref, rt_ref, ct_ref, scale_ref, dt_ref, rise_ref, remain_ref, both_ref, rim_ref,
    x_ref, w_ref, r_ref, i_ref, v_ref, o_ref, gate_ref,
    step_ref, spike_ref, off_ref, rate_ref, pad_ref, sems,
):
    width = x_hbm.shape[2]
    narrow = w_hbm.shape[2]
    broad = i_hbm.shape[2]
    copies = fetch(
        (
            (step_hbm.at[0], step_ref),
            (spike_hbm, spike_ref),
            (off_hbm, off_ref),
            (rate_hbm, rate_ref),
            (w_hbm.at[0], w_ref),
            (wt_hbm, wt_ref),
            (r_hbm.at[0], r_ref),
            (rt_hbm, rt_ref),
            (x_hbm.at[0], x_ref),
            (xt_hbm, xt_ref),
            (gate_hbm.at[0], gate_ref),
            (i_hbm.at[0], i_ref),
            (v_hbm.at[0], v_ref),
            (o_hbm.at[0], o_ref),
            (ct_hbm, ct_ref),
            (scale_hbm, scale_ref),
            (s_hbm, both_ref.at[pl.ds(0, s_hbm.shape[0])]),
            (c_hbm, both_ref.at[pl.ds(s_hbm.shape[0], c_hbm.shape[0])]),
        ),
        sems,
    )
    for copy in copies[:4]:
        copy.wait()
    heads, length = step_ref.shape
    raw = step_ref[...] + column(off_ref[...])
    dt_t = jnp.maximum(raw, 0.0) + jnp.log1p(jnp.exp(-jnp.abs(raw)))
    fall_t = spike_ref[...] - dt_t * column(jnp.exp(rate_ref[...]))
    row = lax.broadcasted_iota(jnp.int32, (length, length), 0)
    col = lax.broadcasted_iota(jnp.int32, (length, length), 1)
    rise_t = jnp.dot(
        fall_t, (row <= col).astype(F32), precision=lax.Precision.HIGHEST, preferred_element_type=F32
    )
    tall = jnp.concatenate([rise_t, dt_t, jnp.zeros((LANES - 2 * heads, length), F32)], axis=0)
    turned_over = jnp.transpose(tall)
    rise = turned_over[:, 0:heads]
    dt = turned_over[:, heads : 2 * heads]
    rise_ref[...] = rise
    dt_ref[...] = dt[0:HEAD, :]
    remain = jnp.exp(jnp.minimum(rise[length - 1 : length, :] - rise, 0.0))
    remain_ref[...] = remain[0:HEAD, :]
    for copy in copies[4:8]:
        copy.wait()
    groups = narrow // STATE
    per_group = width // LANES // groups
    scores = []
    for g in range(groups):
        cols = slice(g * STATE, (g + 1) * STATE)
        write = silu(
            filtered(w_ref[:, cols].astype(F32), wt_ref[:, cols].astype(F32), None, pad_ref)
        ).astype(BF16)
        read = silu(
            filtered(r_ref[:, cols].astype(F32), rt_ref[:, cols].astype(F32), None, pad_ref)
        ).astype(BF16)
        writes_ref[:, cols] = write
        reads_ref[:, cols] = read
        score = lax.dot_general(read, write, (((1,), (1,)), ((), ())), preferred_element_type=F32)
        scores.append(jnp.where(row >= col, score, 0.0))
    for copy in copies[8:10]:
        copy.wait()
    low = lax.broadcasted_iota(jnp.int32, (length, LANES), 1) < HEAD_DIM
    late = lax.broadcasted_iota(jnp.int32, (length, LANES), 0) >= HEAD
    for q in range(width // LANES):
        cols = slice(q * LANES, (q + 1) * LANES)
        x = silu(filtered(x_ref[:, cols].astype(F32), xt_ref[:, cols].astype(F32), None, pad_ref))
        x = x * pair_lanes(dt, q, length)
        weighted_ref[:, cols] = (x * pair_lanes(remain, q, length)).astype(BF16)
        stacked = jnp.concatenate(
            [
                jnp.where(low & late, x, 0.0).astype(BF16),
                jnp.where(late & ~low, x, 0.0).astype(BF16),
            ],
            axis=0,
        )
        both = []
        for h in (2 * q, 2 * q + 1):
            gap = jnp.minimum(rise[:, h : h + 1] - rise_t[h : h + 1, :], 0.0)
            both.append((scores[q // per_group] * jnp.exp(gap)).astype(BF16))
        inside_ref[:, cols] = jnp.dot(
            jnp.concatenate(both, axis=1), stacked, preferred_element_type=F32
        )
    for copy in copies[10:]:
        copy.wait()
    for c in range(0, width, LANES):
        open_ref[:, c : c + LANES] = silu(gate_ref[:, c : c + LANES].astype(F32))
    for c in range(0, broad, LANES):
        cols = slice(c, c + LANES)
        product = i_ref[:, cols].astype(F32) * v_ref[:, cols].astype(F32)
        total = filtered(product, ct_ref[:, cols].astype(F32), None, pad_ref)
        conv_ref[:, cols] = (o_ref[:, cols].astype(F32) * total).astype(BF16)
    at = 0
    for ref in (x_ref, w_ref, r_ref, i_ref, v_ref, o_ref):
        head_ref[:, at : at + ref.shape[1]] = ref[0:HEAD, :]
        if ref is not o_ref:
            rim_ref[:, at : at + ref.shape[1]] = ref[length - RIM : length, :]
        at += ref.shape[1]


def state_kernel(
    rim_ref, weighted_ref, writes_ref, reads_in, inside_in, conv_in, head_ref,
    xt_ref, wt_ref, rt_ref, ct_ref, dt_ref, rise_ref, remain_ref,
    pay_ref, reads_ref, inside_ref, conv_ref, pad_ref,
):
    length, width = weighted_ref.shape
    heads = rise_ref.shape[1]
    narrow = writes_ref.shape[1]
    broad = conv_in.shape[1]
    groups = narrow // STATE
    per_group = width // LANES // groups
    sub = lax.broadcasted_iota(jnp.int32, (EXTRA, LANES), 0)
    rise = rise_ref[...]
    total = rise[length - 1 : length, :]
    dt = dt_ref[...]
    remain = remain_ref[...]
    blocks = STATE // 16

    def first(taps_ref, cols, spot):
        return silu(
            filtered(
                head_ref[:, spot].astype(F32),
                taps_ref[:, cols].astype(F32),
                rim_ref[:, spot].astype(F32),
                pad_ref,
            )
        )

    lane = lax.broadcasted_iota(jnp.int32, (length, LANES), 1)
    row = lax.broadcasted_iota(jnp.int32, (length, LANES), 0)
    share = heads // groups
    for g in range(groups):
        cols = slice(g * STATE, (g + 1) * STATE)
        spot = slice(width + g * STATE, width + (g + 1) * STATE)
        first_write = first(wt_ref, cols, spot).astype(BF16)
        write = jnp.concatenate([first_write, writes_ref[HEAD:, cols]], axis=0)
        write_t = jnp.transpose(write.astype(F32)).astype(BF16)
        firsts = []
        for q in range(g * per_group, (g + 1) * per_group):
            pair = slice(q * LANES, (q + 1) * LANES)
            x = first(xt_ref, pair, pair) * pair_lanes(dt, q, HEAD)
            firsts.append(x.astype(BF16))
            x = (x * pair_lanes(remain, q, HEAD)).astype(BF16)
            weighted = jnp.concatenate([x, weighted_ref[HEAD:, pair]], axis=0)
            state = jnp.dot(write_t, weighted, preferred_element_type=F32)
            pay_ref[q * blocks : (q + 1) * blocks, 0:16, :] = state.reshape(blocks, 16, LANES).astype(BF16)
            t = pair_lanes(total, q, 1)
            hi = t.astype(BF16).astype(F32)
            mid = (t - hi).astype(BF16).astype(F32)
            lo = t - hi - mid
            terms = jnp.where(sub == 0, hi, jnp.where(sub == 1, mid, jnp.where(sub == 2, lo, 0.0))).astype(BF16)
            pay_ref[q * blocks : (q + 1) * blocks, 16 : 16 + EXTRA, :] = jnp.broadcast_to(terms[None], (blocks, EXTRA, LANES))
        spot = slice(width + narrow + g * STATE, width + narrow + (g + 1) * STATE)
        read = jnp.concatenate([first(rt_ref, cols, spot).astype(BF16), reads_in[HEAD:, cols]], axis=0)
        reads_ref[:, cols] = read
        scores = lax.dot_general(
            read, jnp.concatenate([first_write] * share, axis=0), (((1,), (1,)), ((), ())),
            preferred_element_type=F32,
        )
        spread = (
            lax.broadcasted_iota(jnp.int32, (heads, LANES), 0)
            == g * share + lax.broadcasted_iota(jnp.int32, (heads, LANES), 1) // HEAD
        ).astype(F32)
        rises = jnp.dot(rise, spread, precision=lax.Precision.HIGHEST, preferred_element_type=F32)
        here = (row == lane % HEAD)[0:HEAD]
        start = jnp.sum(jnp.where(here, rises[0:HEAD], 0.0), axis=0, keepdims=True)
        kept = jnp.where(
            lane % HEAD <= row, scores * jnp.exp(jnp.minimum(rises - start, 0.0)), 0.0
        ).astype(BF16)
        span = per_group * LANES
        tiled = jnp.concatenate([jnp.concatenate(firsts, axis=1)] * share, axis=0)
        own = (
            lax.broadcasted_iota(jnp.int32, (LANES, span), 0) // HEAD
            == lax.broadcasted_iota(jnp.int32, (LANES, span), 1) // HEAD_DIM
        )
        tiled = jnp.where(own, tiled, jnp.zeros_like(tiled))
        wide = slice(g * span, (g + 1) * span)
        inside_ref[:, wide] = inside_in[:, wide] + jnp.dot(kept, tiled, preferred_element_type=F32)
    base = width + 2 * narrow
    for c in range(0, broad, LANES):
        cols = slice(c, c + LANES)
        i = slice(base + c, base + c + LANES)
        v = slice(base + broad + c, base + broad + c + LANES)
        o = slice(base + 2 * broad + c, base + 2 * broad + c + LANES)
        product = head_ref[:, i].astype(F32) * head_ref[:, v].astype(F32)
        rim = rim_ref[:, i].astype(F32) * rim_ref[:, v].astype(F32)
        value = filtered(product, ct_ref[:, cols].astype(F32), rim, pad_ref)
        conv_ref[0:HEAD, cols] = (head_ref[:, o].astype(F32) * value).astype(BF16)
        conv_ref[HEAD:, cols] = conv_in[HEAD:, cols]


def turned(members, first):
    return [[(k + first) % members for k in range(members)]]


def scan_kernel(in_ref, out_ref):
    members = in_ref.shape[0]
    carry = jnp.zeros((16, LANES), F32)
    for j in range(members):
        at = (j - FIRST_OUT) % members
        out_ref[(j - FIRST_BACK) % members] = carry.astype(BF16)
        if j + 1 < members:
            t = in_ref[at, 16 : 16 + EXTRA, :].astype(F32)
            decay = jnp.exp(t[0:1, :] + t[1:2, :] + t[2:3, :])
            carry = carry * decay + in_ref[at, 0:16, :].astype(F32)


def gate_kernel(p_ref, reads_ref, rise_ref, inside_ref, open_ref, scale_ref, conv_ref, out_ref):
    length, width = inside_ref.shape
    groups = reads_ref.shape[1] // STATE
    per_group = width // LANES // groups
    kept = three(jnp.exp(rise_ref[...]))
    blocks = STATE // 16
    for g in range(groups):
        read = reads_ref[:, g * STATE : (g + 1) * STATE]
        squares = jnp.zeros((length, LANES), F32)
        gated = []
        for q in range(g * per_group, (g + 1) * per_group):
            cols = slice(q * LANES, (q + 1) * LANES)
            spots = [(q * blocks + k + FIRST_OUT - FIRST_BACK) % p_ref.shape[0] for k in range(blocks)]
            before = jnp.concatenate([p_ref[spot] for spot in spots], axis=0)
            carried = jnp.dot(read, before, preferred_element_type=F32)
            y = inside_ref[:, cols] + carried * spread(kept, 2 * q, HEAD_DIM, LANES)
            y = y * open_ref[:, cols]
            squares = squares + y * y
            gated.append(y)
        mean = jnp.sum(squares, axis=1, keepdims=True) * (1.0 / (per_group * LANES))
        inverse = lax.rsqrt(mean + EPS)
        for k, q in enumerate(range(g * per_group, (g + 1) * per_group)):
            cols = slice(q * LANES, (q + 1) * LANES)
            value = (gated[k] * inverse * scale_ref[:, cols]).astype(BF16)
            out_ref[:, cols] = value
    out_ref[:, width:] = conv_ref[...]


def far_kernel(a_ref, w_ref, out_ref):
    out_ref[...] = jnp.dot(a_ref[...], w_ref[...], preferred_element_type=F32).astype(BF16)


def part_kernel(kept, early, first_ref, second_ref, w_ref, out_ref):
    core = lax.axis_index("tp")
    chip = lax.axis_index("fs")
    odd = lax.rem(chip, 2)
    seq = 2 * (core if kept else 1 - core) + (odd if early else 1 - odd)
    away = lax.rem(seq - chip + 4, 4)

    @pl.when(away < 2)
    def _():
        out_ref[...] = jnp.dot(first_ref[...], w_ref[...], preferred_element_type=F32).astype(out_ref.dtype)

    @pl.when(away >= 2)
    def _():
        if early:
            out_ref[...] = second_ref[...].astype(out_ref.dtype)
        else:
            out_ref[...] = jnp.dot(second_ref[...], w_ref[...], preferred_element_type=F32).astype(out_ref.dtype)


def part(kept, early, first, second, rows):
    out = jax.ShapeDtypeStruct((first.shape[0], rows.shape[1]), F32 if kept else BF16)
    return call(functools.partial(part_kernel, kept, early), [out], (first, second, rows))[0]


def merge_kernel(early_ref, early_got_ref, late_ref, late_got_ref, out_ref):
    odd = lax.rem(lax.axis_index("fs"), 2)
    out_ref[odd] = (early_ref[...] + early_got_ref[...].astype(F32)).astype(BF16)
    out_ref[1 - odd] = (late_ref[...] + late_got_ref[...].astype(F32)).astype(BF16)


def per_device(
    output_gate_logits,
    head_input_rows,
    group_state_writes,
    group_state_reads,
    step_logits,
    head_step_offset,
    head_decay_logrates,
    decay_extra_spikes,
    head_input_taps,
    state_input_taps,
    readout_filter_taps,
    grouped_norm_scale,
    convolution_outer_gate,
    convolution_inner_gate,
    convolution_value_rows,
    gated_filter_taps,
    state_output_rows,
    convolution_output_rows,
):
    sds = jax.ShapeDtypeStruct
    _, length, width = head_input_rows.shape
    heads = step_logits.shape[2]
    narrow = group_state_writes.shape[2]
    wide = convolution_inner_gate.shape[2]
    members = lax.axis_size("sp")
    copies = lax.axis_size("fs")
    ends = (
        head_input_rows,
        group_state_writes,
        group_state_reads,
        convolution_inner_gate,
        convolution_value_rows,
    )
    all_width = sum(a.shape[2] for a in ends)
    ins = (
        *ends, convolution_outer_gate, output_gate_logits,
        head_input_taps, state_input_taps, readout_filter_taps, gated_filter_taps,
        grouped_norm_scale[None], jnp.swapaxes(step_logits, 1, 2), decay_extra_spikes.T,
        head_step_offset[None], head_decay_logrates[None], state_output_rows, convolution_output_rows,
    )
    tall = sds((length, width), BF16)
    slim = sds((length, narrow), BF16)
    side = sds((length, wide), BF16)
    full = sds((length, width), F32)
    outs = [
        tall, slim, slim, full, side, full, sds((HEAD, all_width + wide), BF16),
        sds(head_input_taps.shape, BF16), sds(state_input_taps.shape, BF16),
        sds(readout_filter_taps.shape, BF16), sds(gated_filter_taps.shape, BF16),
        sds((1, width), F32), sds((HEAD, heads), F32), sds((length, heads), F32), sds((HEAD, heads), F32),
        sds((width + wide, state_output_rows.shape[1]), BF16), sds((RIM, all_width), BF16),
    ]
    pad = vmem((PAD + length, LANES))
    scratch = [vmem(a.shape[1:], BF16) for a in ins[:7]] + [
        vmem((heads, length)),
        vmem((heads, length)),
        vmem((1, heads)),
        vmem((1, heads)),
        pad,
        sems(18),
    ]
    (
        weighted, writes, reads, inside, conv, opened, head, xt, wt, rt, ct, scale, dt, rise, remain,
        rows_own, rims,
    ) = call(prepare_kernel, outs, ins, 18, scratch)
    before = lax.ppermute(rims, "sp", [(k, k + 1) for k in range(members - 1)])
    ins = (before, weighted, writes, reads, inside, conv, head, xt, wt, rt, ct, dt, rise, remain)
    outs = [sds((members, 16 + EXTRA, LANES), BF16), slim, full, side]
    payload, reads, inside, conv = call(state_kernel, outs, ins, 0, [pad])
    seqs = copies

    def moved(value, away):
        return lax.ppermute(value, "fs", [(k, (k + away) % seqs) for k in range(seqs)])

    rows_far = moved(rows_own, 2)
    gathered = lax.all_to_all(
        payload, "sp", 0, 0, axis_index_groups=turned(members, FIRST_OUT), tiled=True
    )
    prefixes = call(scan_kernel, [sds((members, 16, LANES), BF16)], (gathered,))[0]
    incoming = lax.all_to_all(prefixes, "sp", 0, 0, axis_index_groups=turned(members, FIRST_BACK), tiled=True)
    ins = (incoming, reads, rise, inside, opened, scale, conv)
    own = call(gate_kernel, [sds((length, width + wide), BF16)], ins)[0]
    last = moved(own, 1)
    following = moved(own, -1)
    partial = call(far_kernel, [sds((length, rows_own.shape[1]), BF16)], (own, rows_far))[0]
    far = moved(partial, 2)
    swap = [(0, 1), (1, 0)]
    sent = part(False, True, own, far, rows_own)
    early_got = lax.ppermute(sent, "tp", swap)
    early = part(True, True, own, far, rows_own)
    sent = part(False, False, following, last, rows_own)
    late_got = lax.ppermute(sent, "tp", swap)
    late = part(True, False, following, last, rows_own)
    out = sds((2, length, rows_own.shape[1]), BF16)
    return call(merge_kernel, [out], (early, early_got, late, late_got))[0]


def solution(mesh):
    return jax.shard_map(
        per_device,
        mesh=mesh,
        in_specs=(
            P("fs", "sp", "tp"),
            P("fs", "sp", "tp"),
            P("fs", "sp", "tp"),
            P("fs", "sp", "tp"),
            P("fs", "sp", "tp"),
            P("tp"),
            P("tp"),
            P("sp", "tp"),
            P(None, "tp"),
            P(None, "tp"),
            P(None, "tp"),
            P("tp"),
            P("fs", "sp", "tp"),
            P("fs", "sp", "tp"),
            P("fs", "sp", "tp"),
            P(None, "tp"),
            P("tp", "fs"),
            P("tp", "fs"),
        ),
        out_specs=P("tp", "sp", "fs"),
        check_vma=False,
    )
```

```python
import functools
import itertools

import jax
import jax.numpy as jnp
from jax import lax
from jax.experimental import pallas as pl
from jax.experimental.pallas import tpu as pltpu
from jax.sharding import PartitionSpec as P


EPS = 1e-06
F32 = jnp.float32
BF16 = jnp.bfloat16
STATE = 128
LANES = 128
HEAD_DIM = 64
EXTRA = 8
PAD = 8
RIM = 4
HEAD = 16
SLOTS = 8
LOG2E = 1.4426950408889634
FIRST_OUT = 52
FIRST_BACK = 60


def whole(shape):
    return pl.BlockSpec(shape, lambda *_: (0,) * len(shape))


HBM = pl.BlockSpec(memory_space=pltpu.HBM)


def call(kernel, outs, ins, far=0, scratch=(), flops=50_000_000):
    ins = [pltpu.with_memory_space_constraint(a, pltpu.HBM) for a in ins[:far]] + list(ins[far:])
    return pl.pallas_call(
        kernel,
        grid=(1,),
        in_specs=[HBM] * far + [whole(a.shape) for a in ins[far:]],
        out_specs=[whole(o.shape) for o in outs],
        out_shape=outs,
        scratch_shapes=scratch,
        compiler_params=pltpu.CompilerParams(vmem_limit_bytes=24 * 1024 * 1024),
        cost_estimate=pl.CostEstimate(flops=flops, bytes_accessed=2_000_000, transcendentals=0),
    )(*ins)


def vmem(shape, dtype=F32):
    return pltpu.VMEM(shape, dtype)


def sems(count):
    return pltpu.SemaphoreType.DMA((count,))


def silu(v):
    return v / (1.0 + jnp.exp2(v * -LOG2E))


def pair_lanes(cols, q, rows):
    low = lax.broadcasted_iota(jnp.int32, (rows, LANES), 1) < HEAD_DIM
    first = jnp.broadcast_to(cols[:, 2 * q : 2 * q + 1], (rows, LANES))
    second = jnp.broadcast_to(cols[:, 2 * q + 1 : 2 * q + 2], (rows, LANES))
    return jnp.where(low, first, second)


def three(cols):
    high = cols.astype(BF16)
    rest = cols - high.astype(F32)
    middle = rest.astype(BF16)
    return jnp.concatenate([high, middle, (rest - middle.astype(F32)).astype(BF16)], axis=1)


def spread(parts, first, lanes, width):
    heads = parts.shape[1] // 3
    shape = (parts.shape[1], width)
    wanted = first + (lax.broadcasted_iota(jnp.int32, shape, 1) >> (lanes.bit_length() - 1))
    chosen = (lax.broadcasted_iota(jnp.int32, shape, 0) & (heads - 1)) == wanted
    return jnp.dot(parts, chosen.astype(BF16), preferred_element_type=F32)


def fetch(pairs, sems):
    copies = [pltpu.make_async_copy(src, dst, sems.at[k]) for k, (src, dst) in enumerate(pairs)]
    for copy in copies:
        copy.start()
    return copies


def filtered(rows, taps, rim, pads):
    pad_ref = next(pads)
    length, width = rows.shape
    span = taps.shape[0]
    if rim is None:
        rim = jnp.zeros((RIM, width), F32)
    pad_ref[PAD - RIM : PAD, 0:width] = rim
    pad_ref[PAD : PAD + length, 0:width] = rows
    total = rows * taps[span - 1 : span, :]
    for k in range(span - 1):
        back = span - 1 - k
        total = total + pad_ref[PAD - back : PAD - back + length, 0:width] * taps[k : k + 1, :]
    return total


def column(row):
    size = row.shape[1]
    here = lax.broadcasted_iota(jnp.int32, (size, size), 0) == lax.broadcasted_iota(
        jnp.int32, (size, size), 1
    )
    return jnp.sum(jnp.where(here, jnp.broadcast_to(row, (size, size)), 0.0), axis=1, keepdims=True)


def prepare_kernel(
    x_hbm, w_hbm, r_hbm, i_hbm, v_hbm, o_hbm, gate_hbm, xt_hbm, wt_hbm, rt_hbm, ct_hbm, scale_hbm,
    step_hbm, spike_hbm, off_hbm, rate_hbm, s_hbm, c_hbm,
    weighted_ref, writes_ref, reads_ref, inside_ref, conv_ref, open_ref, head_ref,
    xt_ref, wt_ref, rt_ref, ct_ref, scale_ref, dt_ref, rise_ref, remain_ref, both_ref, rim_ref,
    x_ref, w_ref, r_ref, i_ref, v_ref, o_ref, gate_ref,
    step_ref, spike_ref, off_ref, rate_ref, rises_ref, wide_ref, left_ref, pad_ref, sems,
):
    pads = itertools.cycle([pad_ref.at[k] for k in range(SLOTS)])
    width = x_hbm.shape[2]
    narrow = w_hbm.shape[2]
    broad = i_hbm.shape[2]
    copies = fetch(
        (
            (step_hbm.at[0], step_ref),
            (spike_hbm, spike_ref),
            (off_hbm, off_ref),
            (rate_hbm, rate_ref),
            (w_hbm.at[0], w_ref),
            (wt_hbm, wt_ref),
            (r_hbm.at[0], r_ref),
            (rt_hbm, rt_ref),
            (x_hbm.at[0], x_ref),
            (xt_hbm, xt_ref),
            (gate_hbm.at[0], gate_ref),
            (i_hbm.at[0], i_ref),
            (v_hbm.at[0], v_ref),
            (o_hbm.at[0], o_ref),
            (ct_hbm, ct_ref),
            (scale_hbm, scale_ref),
            (s_hbm, both_ref.at[pl.ds(0, s_hbm.shape[0])]),
            (c_hbm, both_ref.at[pl.ds(s_hbm.shape[0], c_hbm.shape[0])]),
        ),
        sems,
    )
    for copy in copies[:4]:
        copy.wait()
    heads, length = step_ref.shape
    raw = step_ref[...] + column(off_ref[...])
    dt_t = jnp.maximum(raw, 0.0) + jnp.log1p(jnp.exp(-jnp.abs(raw)))
    fall_t = spike_ref[...] - dt_t * column(jnp.exp(rate_ref[...]))
    row = lax.broadcasted_iota(jnp.int32, (length, length), 0)
    col = lax.broadcasted_iota(jnp.int32, (length, length), 1)
    high = fall_t.astype(BF16)
    rest = fall_t - high.astype(F32)
    middle = rest.astype(BF16)
    parts = jnp.concatenate([high, middle, (rest - middle.astype(F32)).astype(BF16)], axis=0)
    sums = jnp.dot(parts, (row <= col).astype(BF16), preferred_element_type=F32)
    rise_t = sums[0:heads] + sums[heads : 2 * heads] + sums[2 * heads :]
    tall = jnp.concatenate([rise_t, dt_t, jnp.zeros((LANES - 2 * heads, length), F32)], axis=0)
    turned_over = jnp.transpose(tall)
    rise = turned_over[:, 0:heads]
    dt = turned_over[:, heads : 2 * heads]
    rise_ref[...] = rise
    dt_ref[...] = dt[0:HEAD, :]
    remain = jnp.exp(jnp.minimum(rise[length - 1 : length, :] - rise, 0.0))
    remain_ref[...] = remain[0:HEAD, :]
    for copy in copies[4:8]:
        copy.wait()
    groups = narrow // STATE
    per_group = width // LANES // groups
    rise2_t = rise_t * LOG2E
    rises_ref[...] = spread(three(rise * LOG2E), 0, LANES, heads * LANES)
    wide_ref[...] = spread(three(dt), 0, HEAD_DIM, width)
    left_ref[...] = spread(three(dt * remain), 0, HEAD_DIM, width)
    scores = []
    for g in range(groups):
        cols = slice(g * STATE, (g + 1) * STATE)
        write = silu(
            filtered(w_ref[:, cols].astype(F32), wt_ref[:, cols].astype(F32), None, pads)
        ).astype(BF16)
        read = silu(
            filtered(r_ref[:, cols].astype(F32), rt_ref[:, cols].astype(F32), None, pads)
        ).astype(BF16)
        writes_ref[:, cols] = write
        reads_ref[:, cols] = read
        score = lax.dot_general(read, write, (((1,), (1,)), ((), ())), preferred_element_type=F32)
        scores.append(jnp.where(row >= col, score, 0.0))
    for copy in copies[8:10]:
        copy.wait()
    low = lax.broadcasted_iota(jnp.int32, (length, LANES), 1) < HEAD_DIM
    late = lax.broadcasted_iota(jnp.int32, (length, LANES), 0) >= HEAD
    for q in range(width // LANES):
        cols = slice(q * LANES, (q + 1) * LANES)
        x = silu(filtered(x_ref[:, cols].astype(F32), xt_ref[:, cols].astype(F32), None, pads))
        weighted_ref[:, cols] = (x * left_ref[:, cols]).astype(BF16)
        x = x * wide_ref[:, cols]
        stacked = jnp.concatenate(
            [
                jnp.where(low & late, x, 0.0).astype(BF16),
                jnp.where(late & ~low, x, 0.0).astype(BF16),
            ],
            axis=0,
        )
        both = []
        for k in range(2):
            h = 2 * q + k
            gap = jnp.minimum(rises_ref[:, h * LANES : (h + 1) * LANES] - rise2_t[h : h + 1, :], 0.0)
            both.append((scores[q // per_group] * jnp.exp2(gap)).astype(BF16))
        inside_ref[:, cols] = jnp.dot(
            jnp.concatenate(both, axis=1), stacked, preferred_element_type=F32
        )
    for copy in copies[10:]:
        copy.wait()
    for c in range(0, width, LANES):
        open_ref[:, c : c + LANES] = silu(gate_ref[:, c : c + LANES].astype(F32))
    for c in range(0, broad, LANES):
        cols = slice(c, c + LANES)
        product = i_ref[:, cols].astype(F32) * v_ref[:, cols].astype(F32)
        total = filtered(product, ct_ref[:, cols].astype(F32), None, pads)
        conv_ref[:, cols] = (o_ref[:, cols].astype(F32) * total).astype(BF16)
    at = 0
    for ref in (x_ref, w_ref, r_ref, i_ref, v_ref, o_ref):
        head_ref[:, at : at + ref.shape[1]] = ref[0:HEAD, :]
        if ref is not o_ref:
            rim_ref[:, at : at + ref.shape[1]] = ref[length - RIM : length, :]
        at += ref.shape[1]


def state_kernel(
    rim_ref, weighted_ref, writes_ref, reads_in, inside_in, conv_in, head_ref,
    xt_ref, wt_ref, rt_ref, ct_ref, dt_ref, rise_ref, remain_ref,
    pay_ref, reads_ref, inside_ref, conv_ref, pad_ref,
):
    pads = itertools.cycle([pad_ref.at[k] for k in range(SLOTS)])
    length, width = weighted_ref.shape
    heads = rise_ref.shape[1]
    narrow = writes_ref.shape[1]
    broad = conv_in.shape[1]
    groups = narrow // STATE
    per_group = width // LANES // groups
    sub = lax.broadcasted_iota(jnp.int32, (EXTRA, LANES), 0)
    rise = rise_ref[...]
    total = rise[length - 1 : length, :]
    dt = dt_ref[...]
    remain = remain_ref[...]
    blocks = STATE // 16

    def first(taps_ref, cols, spot):
        return silu(
            filtered(
                head_ref[:, spot].astype(F32),
                taps_ref[:, cols].astype(F32),
                rim_ref[:, spot].astype(F32),
                pads,
            )
        )

    lane = lax.broadcasted_iota(jnp.int32, (length, LANES), 1)
    row = lax.broadcasted_iota(jnp.int32, (length, LANES), 0)
    share = heads // groups
    rise_parts = three(rise)
    for g in range(groups):
        cols = slice(g * STATE, (g + 1) * STATE)
        spot = slice(width + g * STATE, width + (g + 1) * STATE)
        first_write = first(wt_ref, cols, spot).astype(BF16)
        write = jnp.concatenate([first_write, writes_ref[HEAD:, cols]], axis=0)
        write_t = jnp.transpose(write.astype(F32)).astype(BF16)
        firsts = []
        for q in range(g * per_group, (g + 1) * per_group):
            pair = slice(q * LANES, (q + 1) * LANES)
            x = first(xt_ref, pair, pair) * pair_lanes(dt, q, HEAD)
            firsts.append(x.astype(BF16))
            x = (x * pair_lanes(remain, q, HEAD)).astype(BF16)
            weighted = jnp.concatenate([x, weighted_ref[HEAD:, pair]], axis=0)
            state = jnp.dot(write_t, weighted, preferred_element_type=F32)
            pay_ref[q * blocks : (q + 1) * blocks, 0:16, :] = state.reshape(blocks, 16, LANES).astype(BF16)
            t = pair_lanes(total, q, 1)
            hi = t.astype(BF16).astype(F32)
            mid = (t - hi).astype(BF16).astype(F32)
            lo = t - hi - mid
            terms = jnp.where(sub == 0, hi, jnp.where(sub == 1, mid, jnp.where(sub == 2, lo, 0.0))).astype(BF16)
            pay_ref[q * blocks : (q + 1) * blocks, 16 : 16 + EXTRA, :] = jnp.broadcast_to(terms[None], (blocks, EXTRA, LANES))
        spot = slice(width + narrow + g * STATE, width + narrow + (g + 1) * STATE)
        read = jnp.concatenate([first(rt_ref, cols, spot).astype(BF16), reads_in[HEAD:, cols]], axis=0)
        reads_ref[:, cols] = read
        scores = lax.dot_general(
            read, jnp.concatenate([first_write] * share, axis=0), (((1,), (1,)), ((), ())),
            preferred_element_type=F32,
        )
        rises = spread(rise_parts, g * share, HEAD, LANES)
        here = (row == (lane & (HEAD - 1)))[0:HEAD]
        start = jnp.sum(jnp.where(here, rises[0:HEAD], 0.0), axis=0, keepdims=True)
        kept = jnp.where(
            (lane & (HEAD - 1)) <= row, scores * jnp.exp(jnp.minimum(rises - start, 0.0)), 0.0
        ).astype(BF16)
        span = per_group * LANES
        tiled = jnp.concatenate([jnp.concatenate(firsts, axis=1)] * share, axis=0)
        own = (
            lax.broadcasted_iota(jnp.int32, (LANES, span), 0) >> (HEAD.bit_length() - 1)
            == lax.broadcasted_iota(jnp.int32, (LANES, span), 1) >> (HEAD_DIM.bit_length() - 1)
        )
        tiled = jnp.where(own, tiled, jnp.zeros_like(tiled))
        wide = slice(g * span, (g + 1) * span)
        inside_ref[:, wide] = inside_in[:, wide] + jnp.dot(kept, tiled, preferred_element_type=F32)
    base = width + 2 * narrow
    for c in range(0, broad, LANES):
        cols = slice(c, c + LANES)
        i = slice(base + c, base + c + LANES)
        v = slice(base + broad + c, base + broad + c + LANES)
        o = slice(base + 2 * broad + c, base + 2 * broad + c + LANES)
        product = head_ref[:, i].astype(F32) * head_ref[:, v].astype(F32)
        rim = rim_ref[:, i].astype(F32) * rim_ref[:, v].astype(F32)
        value = filtered(product, ct_ref[:, cols].astype(F32), rim, pads)
        conv_ref[0:HEAD, cols] = (head_ref[:, o].astype(F32) * value).astype(BF16)
        conv_ref[HEAD:, cols] = conv_in[HEAD:, cols]


def turned(members, first):
    return [[(k + first) % members for k in range(members)]]


def scan_kernel(in_ref, out_ref):
    members = in_ref.shape[0]
    carry = jnp.zeros((16, LANES), F32)
    for j in range(members):
        at = (j - FIRST_OUT) % members
        out_ref[(j - FIRST_BACK) % members] = carry.astype(BF16)
        if j + 1 < members:
            t = in_ref[at, 16 : 16 + EXTRA, :].astype(F32)
            decay = jnp.exp(t[0:1, :] + t[1:2, :] + t[2:3, :])
            carry = carry * decay + in_ref[at, 0:16, :].astype(F32)


def gate_kernel(p_ref, reads_ref, rise_ref, inside_ref, open_ref, scale_ref, conv_ref, out_ref):
    length, width = inside_ref.shape
    groups = reads_ref.shape[1] // STATE
    per_group = width // LANES // groups
    kept = three(jnp.exp(rise_ref[...]))
    blocks = STATE // 16
    for g in range(groups):
        read = reads_ref[:, g * STATE : (g + 1) * STATE]
        squares = jnp.zeros((length, LANES), F32)
        gated = []
        for q in range(g * per_group, (g + 1) * per_group):
            cols = slice(q * LANES, (q + 1) * LANES)
            spots = [(q * blocks + k + FIRST_OUT - FIRST_BACK) % p_ref.shape[0] for k in range(blocks)]
            before = jnp.concatenate([p_ref[spot] for spot in spots], axis=0)
            carried = jnp.dot(read, before, preferred_element_type=F32)
            y = inside_ref[:, cols] + carried * spread(kept, 2 * q, HEAD_DIM, LANES)
            y = y * open_ref[:, cols]
            squares = squares + y * y
            gated.append(y)
        mean = jnp.sum(squares, axis=1, keepdims=True) * (1.0 / (per_group * LANES))
        inverse = lax.rsqrt(mean + EPS)
        for k, q in enumerate(range(g * per_group, (g + 1) * per_group)):
            cols = slice(q * LANES, (q + 1) * LANES)
            value = (gated[k] * inverse * scale_ref[:, cols]).astype(BF16)
            out_ref[:, cols] = value
    out_ref[:, width:] = conv_ref[...]


def far_kernel(a_ref, w_ref, out_ref):
    out_ref[...] = jnp.dot(a_ref[...], w_ref[...], preferred_element_type=F32).astype(BF16)


def part_kernel(kept, early, first_ref, second_ref, w_ref, out_ref):
    core = lax.axis_index("tp")
    chip = lax.axis_index("fs")
    odd = lax.rem(chip, 2)
    seq = 2 * (core if kept else 1 - core) + (odd if early else 1 - odd)
    away = lax.rem(seq - chip + 4, 4)

    @pl.when(away < 2)
    def _():
        out_ref[...] = jnp.dot(first_ref[...], w_ref[...], preferred_element_type=F32).astype(out_ref.dtype)

    @pl.when(away >= 2)
    def _():
        if early:
            out_ref[...] = second_ref[...].astype(out_ref.dtype)
        else:
            out_ref[...] = jnp.dot(second_ref[...], w_ref[...], preferred_element_type=F32).astype(out_ref.dtype)


def part(kept, early, first, second, rows):
    out = jax.ShapeDtypeStruct((first.shape[0], rows.shape[1]), F32 if kept else BF16)
    return call(functools.partial(part_kernel, kept, early), [out], (first, second, rows))[0]


def merge_kernel(early_ref, early_got_ref, late_ref, late_got_ref, out_ref):
    odd = lax.rem(lax.axis_index("fs"), 2)
    out_ref[odd] = (early_ref[...] + early_got_ref[...].astype(F32)).astype(BF16)
    out_ref[1 - odd] = (late_ref[...] + late_got_ref[...].astype(F32)).astype(BF16)


def per_device(
    output_gate_logits,
    head_input_rows,
    group_state_writes,
    group_state_reads,
    step_logits,
    head_step_offset,
    head_decay_logrates,
    decay_extra_spikes,
    head_input_taps,
    state_input_taps,
    readout_filter_taps,
    grouped_norm_scale,
    convolution_outer_gate,
    convolution_inner_gate,
    convolution_value_rows,
    gated_filter_taps,
    state_output_rows,
    convolution_output_rows,
):
    sds = jax.ShapeDtypeStruct
    _, length, width = head_input_rows.shape
    heads = step_logits.shape[2]
    narrow = group_state_writes.shape[2]
    wide = convolution_inner_gate.shape[2]
    members = lax.axis_size("sp")
    copies = lax.axis_size("fs")
    ends = (
        head_input_rows,
        group_state_writes,
        group_state_reads,
        convolution_inner_gate,
        convolution_value_rows,
    )
    all_width = sum(a.shape[2] for a in ends)
    ins = (
        *ends, convolution_outer_gate, output_gate_logits,
        head_input_taps, state_input_taps, readout_filter_taps, gated_filter_taps,
        grouped_norm_scale[None], jnp.swapaxes(step_logits, 1, 2), decay_extra_spikes.T,
        head_step_offset[None], head_decay_logrates[None], state_output_rows, convolution_output_rows,
    )
    tall = sds((length, width), BF16)
    slim = sds((length, narrow), BF16)
    side = sds((length, wide), BF16)
    full = sds((length, width), F32)
    outs = [
        tall, slim, slim, full, side, full, sds((HEAD, all_width + wide), BF16),
        sds(head_input_taps.shape, BF16), sds(state_input_taps.shape, BF16),
        sds(readout_filter_taps.shape, BF16), sds(gated_filter_taps.shape, BF16),
        sds((1, width), F32), sds((HEAD, heads), F32), sds((length, heads), F32), sds((HEAD, heads), F32),
        sds((width + wide, state_output_rows.shape[1]), BF16), sds((RIM, all_width), BF16),
    ]
    pad = vmem((SLOTS, PAD + length, LANES))
    scratch = [vmem(a.shape[1:], BF16) for a in ins[:7]] + [
        vmem((heads, length)),
        vmem((heads, length)),
        vmem((1, heads)),
        vmem((1, heads)),
        vmem((length, heads * LANES)),
        vmem((length, width)),
        vmem((length, width)),
        pad,
        sems(18),
    ]
    (
        weighted, writes, reads, inside, conv, opened, head, xt, wt, rt, ct, scale, dt, rise, remain,
        rows_own, rims,
    ) = call(prepare_kernel, outs, ins, 18, scratch)
    before = lax.ppermute(rims, "sp", [(k, k + 1) for k in range(members - 1)])
    ins = (before, weighted, writes, reads, inside, conv, head, xt, wt, rt, ct, dt, rise, remain)
    outs = [sds((members, 16 + EXTRA, LANES), BF16), slim, full, side]
    payload, reads, inside, conv = call(state_kernel, outs, ins, 0, [pad])
    seqs = copies

    def moved(value, away):
        return lax.ppermute(value, "fs", [(k, (k + away) % seqs) for k in range(seqs)])

    rows_far = moved(rows_own, 2)
    gathered = lax.all_to_all(
        payload, "sp", 0, 0, axis_index_groups=turned(members, FIRST_OUT), tiled=True
    )
    prefixes = call(scan_kernel, [sds((members, 16, LANES), BF16)], (gathered,))[0]
    incoming = lax.all_to_all(prefixes, "sp", 0, 0, axis_index_groups=turned(members, FIRST_BACK), tiled=True)
    ins = (incoming, reads, rise, inside, opened, scale, conv)
    own = call(gate_kernel, [sds((length, width + wide), BF16)], ins)[0]
    last = moved(own, 1)
    following = moved(own, -1)
    partial = call(far_kernel, [sds((length, rows_own.shape[1]), BF16)], (own, rows_far))[0]
    far = moved(partial, 2)
    swap = [(0, 1), (1, 0)]
    sent = part(False, True, own, far, rows_own)
    early_got = lax.ppermute(sent, "tp", swap)
    early = part(True, True, own, far, rows_own)
    sent = part(False, False, following, last, rows_own)
    late_got = lax.ppermute(sent, "tp", swap)
    late = part(True, False, following, last, rows_own)
    out = sds((2, length, rows_own.shape[1]), BF16)
    return call(merge_kernel, [out], (early, early_got, late, late_got))[0]


def solution(mesh):
    return jax.shard_map(
        per_device,
        mesh=mesh,
        in_specs=(
            P("fs", "sp", "tp"),
            P("fs", "sp", "tp"),
            P("fs", "sp", "tp"),
            P("fs", "sp", "tp"),
            P("fs", "sp", "tp"),
            P("tp"),
            P("tp"),
            P("sp", "tp"),
            P(None, "tp"),
            P(None, "tp"),
            P(None, "tp"),
            P("tp"),
            P("fs", "sp", "tp"),
            P("fs", "sp", "tp"),
            P("fs", "sp", "tp"),
            P(None, "tp"),
            P("tp", "fs"),
            P("tp", "fs"),
        ),
        out_specs=P("tp", "sp", "fs"),
        check_vma=False,
    )
```

```python
import functools
import itertools

import jax
import jax.numpy as jnp
from jax import lax
from jax.experimental import pallas as pl
from jax.experimental.pallas import tpu as pltpu
from jax.sharding import PartitionSpec as P


EPS = 1e-06
F32 = jnp.float32
BF16 = jnp.bfloat16
STATE = 128
LANES = 128
HEAD_DIM = 64
EXTRA = 8
PAD = 8
RIM = 4
HEAD = 16
SLOTS = 8
LOG2E = 1.4426950408889634
FIRST_OUT = 52
FIRST_BACK = 60


def whole(shape):
    return pl.BlockSpec(shape, lambda *_: (0,) * len(shape))


HBM = pl.BlockSpec(memory_space=pltpu.HBM)


def call(kernel, outs, ins, far=0, scratch=(), flops=50_000_000):
    ins = [pltpu.with_memory_space_constraint(a, pltpu.HBM) for a in ins[:far]] + list(ins[far:])
    return pl.pallas_call(
        kernel,
        grid=(1,),
        in_specs=[HBM] * far + [whole(a.shape) for a in ins[far:]],
        out_specs=[whole(o.shape) for o in outs],
        out_shape=outs,
        scratch_shapes=scratch,
        compiler_params=pltpu.CompilerParams(vmem_limit_bytes=24 * 1024 * 1024),
        cost_estimate=pl.CostEstimate(flops=flops, bytes_accessed=2_000_000, transcendentals=0),
    )(*ins)


def vmem(shape, dtype=F32):
    return pltpu.VMEM(shape, dtype)


def sems(count):
    return pltpu.SemaphoreType.DMA((count,))


def silu(v):
    return v / (1.0 + jnp.exp2(v * -LOG2E))


def pair_lanes(cols, q, rows):
    low = lax.broadcasted_iota(jnp.int32, (rows, LANES), 1) < HEAD_DIM
    first = jnp.broadcast_to(cols[:, 2 * q : 2 * q + 1], (rows, LANES))
    second = jnp.broadcast_to(cols[:, 2 * q + 1 : 2 * q + 2], (rows, LANES))
    return jnp.where(low, first, second)


def three(cols):
    high = cols.astype(BF16)
    rest = cols - high.astype(F32)
    middle = rest.astype(BF16)
    return jnp.concatenate([high, middle, (rest - middle.astype(F32)).astype(BF16)], axis=1)


def spread(parts, first, lanes, width):
    heads = parts.shape[1] // 3
    shape = (parts.shape[1], width)
    wanted = first + (lax.broadcasted_iota(jnp.int32, shape, 1) >> (lanes.bit_length() - 1))
    chosen = (lax.broadcasted_iota(jnp.int32, shape, 0) & (heads - 1)) == wanted
    return jnp.dot(parts, chosen.astype(BF16), preferred_element_type=F32)


def fetch(pairs, sems):
    copies = [pltpu.make_async_copy(src, dst, sems.at[k]) for k, (src, dst) in enumerate(pairs)]
    for copy in copies:
        copy.start()
    return copies


def filtered(rows, taps, rim, pads):
    pad_ref = next(pads)
    length, width = rows.shape
    span = taps.shape[0]
    if rim is None:
        rim = jnp.zeros((RIM, width), F32)
    pad_ref[PAD - RIM : PAD, 0:width] = rim
    pad_ref[PAD : PAD + length, 0:width] = rows
    total = rows * taps[span - 1 : span, :]
    for k in range(span - 1):
        back = span - 1 - k
        total = total + pad_ref[PAD - back : PAD - back + length, 0:width] * taps[k : k + 1, :]
    return total


def column(row):
    size = row.shape[1]
    here = lax.broadcasted_iota(jnp.int32, (size, size), 0) == lax.broadcasted_iota(
        jnp.int32, (size, size), 1
    )
    return jnp.sum(jnp.where(here, jnp.broadcast_to(row, (size, size)), 0.0), axis=1, keepdims=True)


def prepare_kernel(
    x_hbm, w_hbm, r_hbm, i_hbm, v_hbm, o_hbm, gate_hbm, xt_hbm, wt_hbm, rt_hbm, ct_hbm, scale_hbm,
    step_hbm, spike_hbm, off_hbm, rate_hbm, s_hbm, c_hbm,
    weighted_ref, writes_ref, reads_ref, inside_ref, conv_ref, open_ref, head_ref,
    xt_ref, wt_ref, rt_ref, ct_ref, scale_ref, dt_ref, rise_ref, remain_ref, both_ref, rim_ref,
    x_ref, w_ref, r_ref, i_ref, v_ref, o_ref, gate_ref,
    step_ref, spike_ref, off_ref, rate_ref, rises_ref, wide_ref, left_ref, pad_ref, sems,
):
    pads = itertools.cycle([pad_ref.at[k] for k in range(SLOTS)])
    width = x_hbm.shape[2]
    narrow = w_hbm.shape[2]
    broad = i_hbm.shape[2]
    copies = fetch(
        (
            (step_hbm.at[0], step_ref),
            (spike_hbm, spike_ref),
            (off_hbm, off_ref),
            (rate_hbm, rate_ref),
            (w_hbm.at[0], w_ref),
            (wt_hbm, wt_ref),
            (r_hbm.at[0], r_ref),
            (rt_hbm, rt_ref),
            (x_hbm.at[0], x_ref),
            (xt_hbm, xt_ref),
            (gate_hbm.at[0], gate_ref),
            (i_hbm.at[0], i_ref),
            (v_hbm.at[0], v_ref),
            (o_hbm.at[0], o_ref),
            (ct_hbm, ct_ref),
            (scale_hbm, scale_ref),
            (s_hbm, both_ref.at[pl.ds(0, s_hbm.shape[0])]),
            (c_hbm, both_ref.at[pl.ds(s_hbm.shape[0], c_hbm.shape[0])]),
        ),
        sems,
    )
    for copy in copies[:4]:
        copy.wait()
    heads, length = step_ref.shape
    raw = step_ref[...] + column(off_ref[...])
    dt_t = jnp.maximum(raw, 0.0) + jnp.log1p(jnp.exp(-jnp.abs(raw)))
    fall_t = spike_ref[...] - dt_t * column(jnp.exp(rate_ref[...]))
    row = lax.broadcasted_iota(jnp.int32, (length, length), 0)
    col = lax.broadcasted_iota(jnp.int32, (length, length), 1)
    high = fall_t.astype(BF16)
    rest = fall_t - high.astype(F32)
    middle = rest.astype(BF16)
    parts = jnp.concatenate([high, middle, (rest - middle.astype(F32)).astype(BF16)], axis=0)
    sums = jnp.dot(parts, (row <= col).astype(BF16), preferred_element_type=F32)
    rise_t = sums[0:heads] + sums[heads : 2 * heads] + sums[2 * heads :]
    tall = jnp.concatenate([rise_t, dt_t, jnp.zeros((LANES - 2 * heads, length), F32)], axis=0)
    turned_over = jnp.transpose(tall)
    rise = turned_over[:, 0:heads]
    dt = turned_over[:, heads : 2 * heads]
    rise_ref[...] = rise
    dt_ref[...] = dt[0:HEAD, :]
    remain = jnp.exp(jnp.minimum(rise[length - 1 : length, :] - rise, 0.0))
    remain_ref[...] = remain[0:HEAD, :]
    for copy in copies[4:8]:
        copy.wait()
    groups = narrow // STATE
    per_group = width // LANES // groups
    rise2_t = rise_t * LOG2E
    rises_ref[...] = spread(three(rise * LOG2E), 0, LANES, heads * LANES)
    wide_ref[...] = spread(three(dt), 0, HEAD_DIM, width)
    left_ref[...] = spread(three(dt * remain), 0, HEAD_DIM, width)
    scores = []
    for g in range(groups):
        cols = slice(g * STATE, (g + 1) * STATE)
        write = silu(
            filtered(w_ref[:, cols].astype(F32), wt_ref[:, cols].astype(F32), None, pads)
        ).astype(BF16)
        read = silu(
            filtered(r_ref[:, cols].astype(F32), rt_ref[:, cols].astype(F32), None, pads)
        ).astype(BF16)
        writes_ref[:, cols] = write
        reads_ref[:, cols] = read
        score = lax.dot_general(read, write, (((1,), (1,)), ((), ())), preferred_element_type=F32)
        scores.append(jnp.where(row >= col, score, 0.0))
    for copy in copies[8:10]:
        copy.wait()
    low = lax.broadcasted_iota(jnp.int32, (length, LANES), 1) < HEAD_DIM
    late = lax.broadcasted_iota(jnp.int32, (length, LANES), 0) >= HEAD
    for q in range(width // LANES):
        cols = slice(q * LANES, (q + 1) * LANES)
        x = silu(filtered(x_ref[:, cols].astype(F32), xt_ref[:, cols].astype(F32), None, pads))
        weighted_ref[:, cols] = (x * left_ref[:, cols]).astype(BF16)
        x = x * wide_ref[:, cols]
        stacked = jnp.concatenate(
            [
                jnp.where(low & late, x, 0.0).astype(BF16),
                jnp.where(late & ~low, x, 0.0).astype(BF16),
            ],
            axis=0,
        )
        both = []
        for k in range(2):
            h = 2 * q + k
            gap = jnp.minimum(rises_ref[:, h * LANES : (h + 1) * LANES] - rise2_t[h : h + 1, :], 0.0)
            both.append((scores[q // per_group] * jnp.exp2(gap)).astype(BF16))
        inside_ref[:, cols] = jnp.dot(
            jnp.concatenate(both, axis=1), stacked, preferred_element_type=F32
        )
    for copy in copies[10:]:
        copy.wait()
    for c in range(0, width, LANES):
        open_ref[:, c : c + LANES] = silu(gate_ref[:, c : c + LANES].astype(F32))
    for c in range(0, broad, LANES):
        cols = slice(c, c + LANES)
        product = i_ref[:, cols].astype(F32) * v_ref[:, cols].astype(F32)
        total = filtered(product, ct_ref[:, cols].astype(F32), None, pads)
        conv_ref[:, cols] = (o_ref[:, cols].astype(F32) * total).astype(BF16)
    at = 0
    for ref in (x_ref, w_ref, r_ref, i_ref, v_ref, o_ref):
        head_ref[:, at : at + ref.shape[1]] = ref[0:HEAD, :]
        if ref is not o_ref:
            rim_ref[:, at : at + ref.shape[1]] = ref[length - RIM : length, :]
        at += ref.shape[1]


def state_kernel(
    rim_ref, weighted_ref, writes_ref, reads_in, inside_in, conv_in, head_ref,
    xt_ref, wt_ref, rt_ref, ct_ref, dt_ref, rise_ref, remain_ref,
    pay_ref, reads_ref, inside_ref, conv_ref, pad_ref,
):
    pads = itertools.cycle([pad_ref.at[k] for k in range(SLOTS)])
    length, width = weighted_ref.shape
    heads = rise_ref.shape[1]
    narrow = writes_ref.shape[1]
    broad = conv_in.shape[1]
    groups = narrow // STATE
    per_group = width // LANES // groups
    sub = lax.broadcasted_iota(jnp.int32, (EXTRA, LANES), 0)
    rise = rise_ref[...]
    total = rise[length - 1 : length, :]
    dt = dt_ref[...]
    remain = remain_ref[...]
    blocks = STATE // 16

    def first(taps_ref, cols, spot):
        return silu(
            filtered(
                head_ref[:, spot].astype(F32),
                taps_ref[:, cols].astype(F32),
                rim_ref[:, spot].astype(F32),
                pads,
            )
        )

    lane = lax.broadcasted_iota(jnp.int32, (length, LANES), 1)
    row = lax.broadcasted_iota(jnp.int32, (length, LANES), 0)
    share = heads // groups
    rise_parts = three(rise)
    for g in range(groups):
        cols = slice(g * STATE, (g + 1) * STATE)
        spot = slice(width + g * STATE, width + (g + 1) * STATE)
        first_write = first(wt_ref, cols, spot).astype(BF16)
        write = jnp.concatenate([first_write, writes_ref[HEAD:, cols]], axis=0)
        write_t = jnp.transpose(write.astype(F32)).astype(BF16)
        firsts = []
        for q in range(g * per_group, (g + 1) * per_group):
            pair = slice(q * LANES, (q + 1) * LANES)
            x = first(xt_ref, pair, pair) * pair_lanes(dt, q, HEAD)
            firsts.append(x.astype(BF16))
            x = (x * pair_lanes(remain, q, HEAD)).astype(BF16)
            weighted = jnp.concatenate([x, weighted_ref[HEAD:, pair]], axis=0)
            state = jnp.dot(write_t, weighted, preferred_element_type=F32)
            pay_ref[q * blocks : (q + 1) * blocks, 0:16, :] = state.reshape(blocks, 16, LANES).astype(BF16)
            t = pair_lanes(total, q, 1)
            hi = t.astype(BF16).astype(F32)
            mid = (t - hi).astype(BF16).astype(F32)
            lo = t - hi - mid
            terms = jnp.where(sub == 0, hi, jnp.where(sub == 1, mid, jnp.where(sub == 2, lo, 0.0))).astype(BF16)
            pay_ref[q * blocks : (q + 1) * blocks, 16 : 16 + EXTRA, :] = jnp.broadcast_to(terms[None], (blocks, EXTRA, LANES))
        spot = slice(width + narrow + g * STATE, width + narrow + (g + 1) * STATE)
        read = jnp.concatenate([first(rt_ref, cols, spot).astype(BF16), reads_in[HEAD:, cols]], axis=0)
        reads_ref[:, cols] = read
        scores = lax.dot_general(
            read, jnp.concatenate([first_write] * share, axis=0), (((1,), (1,)), ((), ())),
            preferred_element_type=F32,
        )
        rises = spread(rise_parts, g * share, HEAD, LANES)
        here = (row == (lane & (HEAD - 1)))[0:HEAD]
        start = jnp.sum(jnp.where(here, rises[0:HEAD], 0.0), axis=0, keepdims=True)
        kept = jnp.where(
            (lane & (HEAD - 1)) <= row, scores * jnp.exp(jnp.minimum(rises - start, 0.0)), 0.0
        ).astype(BF16)
        span = per_group * LANES
        tiled = jnp.concatenate([jnp.concatenate(firsts, axis=1)] * share, axis=0)
        own = (
            lax.broadcasted_iota(jnp.int32, (LANES, span), 0) >> (HEAD.bit_length() - 1)
            == lax.broadcasted_iota(jnp.int32, (LANES, span), 1) >> (HEAD_DIM.bit_length() - 1)
        )
        tiled = jnp.where(own, tiled, jnp.zeros_like(tiled))
        wide = slice(g * span, (g + 1) * span)
        inside_ref[:, wide] = inside_in[:, wide] + jnp.dot(kept, tiled, preferred_element_type=F32)
    base = width + 2 * narrow
    for c in range(0, broad, LANES):
        cols = slice(c, c + LANES)
        i = slice(base + c, base + c + LANES)
        v = slice(base + broad + c, base + broad + c + LANES)
        o = slice(base + 2 * broad + c, base + 2 * broad + c + LANES)
        product = head_ref[:, i].astype(F32) * head_ref[:, v].astype(F32)
        rim = rim_ref[:, i].astype(F32) * rim_ref[:, v].astype(F32)
        value = filtered(product, ct_ref[:, cols].astype(F32), rim, pads)
        conv_ref[0:HEAD, cols] = (head_ref[:, o].astype(F32) * value).astype(BF16)
        conv_ref[HEAD:, cols] = conv_in[HEAD:, cols]


def turned(members, first):
    return [[(k + first) % members for k in range(members)]]


def scan_kernel(in_ref, out_ref):
    members = in_ref.shape[0]
    carry = jnp.zeros((16, LANES), F32)
    for j in range(members):
        at = (j - FIRST_OUT) % members
        out_ref[(j - FIRST_BACK) % members] = carry.astype(BF16)
        if j + 1 < members:
            t = in_ref[at, 16 : 16 + EXTRA, :].astype(F32)
            decay = jnp.exp(t[0:1, :] + t[1:2, :] + t[2:3, :])
            carry = carry * decay + in_ref[at, 0:16, :].astype(F32)


def gate_kernel(p_ref, reads_ref, rise_ref, inside_ref, open_ref, scale_ref, conv_ref, out_ref, kept_ref):
    length, width = inside_ref.shape
    groups = reads_ref.shape[1] // STATE
    per_group = width // LANES // groups
    kept_ref[...] = spread(three(jnp.exp(rise_ref[...])), 0, HEAD_DIM, width)
    blocks = STATE // 16
    for g in range(groups):
        read = reads_ref[:, g * STATE : (g + 1) * STATE]
        squares = jnp.zeros((length, LANES), F32)
        gated = []
        for q in range(g * per_group, (g + 1) * per_group):
            cols = slice(q * LANES, (q + 1) * LANES)
            spots = [(q * blocks + k + FIRST_OUT - FIRST_BACK) % p_ref.shape[0] for k in range(blocks)]
            before = jnp.concatenate([p_ref[spot] for spot in spots], axis=0)
            carried = jnp.dot(read, before, preferred_element_type=F32)
            y = inside_ref[:, cols] + carried * kept_ref[:, cols]
            y = y * open_ref[:, cols]
            squares = squares + y * y
            gated.append(y)
        mean = jnp.sum(squares, axis=1, keepdims=True) * (1.0 / (per_group * LANES))
        inverse = lax.rsqrt(mean + EPS)
        for k, q in enumerate(range(g * per_group, (g + 1) * per_group)):
            cols = slice(q * LANES, (q + 1) * LANES)
            value = (gated[k] * inverse * scale_ref[:, cols]).astype(BF16)
            out_ref[:, cols] = value
    out_ref[:, width:] = conv_ref[...]


def far_kernel(a_ref, w_ref, out_ref):
    out_ref[...] = jnp.dot(a_ref[...], w_ref[...], preferred_element_type=F32).astype(BF16)


def part_kernel(kept, early, first_ref, second_ref, w_ref, out_ref):
    core = lax.axis_index("tp")
    chip = lax.axis_index("fs")
    odd = lax.rem(chip, 2)
    seq = 2 * (core if kept else 1 - core) + (odd if early else 1 - odd)
    away = lax.rem(seq - chip + 4, 4)

    @pl.when(away < 2)
    def _():
        out_ref[...] = jnp.dot(first_ref[...], w_ref[...], preferred_element_type=F32).astype(out_ref.dtype)

    @pl.when(away >= 2)
    def _():
        if early:
            out_ref[...] = second_ref[...].astype(out_ref.dtype)
        else:
            out_ref[...] = jnp.dot(second_ref[...], w_ref[...], preferred_element_type=F32).astype(out_ref.dtype)


def part(kept, early, first, second, rows):
    out = jax.ShapeDtypeStruct((first.shape[0], rows.shape[1]), F32 if kept else BF16)
    return call(functools.partial(part_kernel, kept, early), [out], (first, second, rows))[0]


def merge_kernel(early_ref, early_got_ref, late_ref, late_got_ref, out_ref):
    odd = lax.rem(lax.axis_index("fs"), 2)
    out_ref[odd] = (early_ref[...] + early_got_ref[...].astype(F32)).astype(BF16)
    out_ref[1 - odd] = (late_ref[...] + late_got_ref[...].astype(F32)).astype(BF16)


def per_device(
    output_gate_logits,
    head_input_rows,
    group_state_writes,
    group_state_reads,
    step_logits,
    head_step_offset,
    head_decay_logrates,
    decay_extra_spikes,
    head_input_taps,
    state_input_taps,
    readout_filter_taps,
    grouped_norm_scale,
    convolution_outer_gate,
    convolution_inner_gate,
    convolution_value_rows,
    gated_filter_taps,
    state_output_rows,
    convolution_output_rows,
):
    sds = jax.ShapeDtypeStruct
    _, length, width = head_input_rows.shape
    heads = step_logits.shape[2]
    narrow = group_state_writes.shape[2]
    wide = convolution_inner_gate.shape[2]
    members = lax.axis_size("sp")
    copies = lax.axis_size("fs")
    ends = (
        head_input_rows,
        group_state_writes,
        group_state_reads,
        convolution_inner_gate,
        convolution_value_rows,
    )
    all_width = sum(a.shape[2] for a in ends)
    ins = (
        *ends, convolution_outer_gate, output_gate_logits,
        head_input_taps, state_input_taps, readout_filter_taps, gated_filter_taps,
        grouped_norm_scale[None], jnp.swapaxes(step_logits, 1, 2), decay_extra_spikes.T,
        head_step_offset[None], head_decay_logrates[None], state_output_rows, convolution_output_rows,
    )
    tall = sds((length, width), BF16)
    slim = sds((length, narrow), BF16)
    side = sds((length, wide), BF16)
    full = sds((length, width), F32)
    outs = [
        tall, slim, slim, full, side, full, sds((HEAD, all_width + wide), BF16),
        sds(head_input_taps.shape, BF16), sds(state_input_taps.shape, BF16),
        sds(readout_filter_taps.shape, BF16), sds(gated_filter_taps.shape, BF16),
        sds((1, width), F32), sds((HEAD, heads), F32), sds((length, heads), F32), sds((HEAD, heads), F32),
        sds((width + wide, state_output_rows.shape[1]), BF16), sds((RIM, all_width), BF16),
    ]
    pad = vmem((SLOTS, PAD + length, LANES))
    scratch = [vmem(a.shape[1:], BF16) for a in ins[:7]] + [
        vmem((heads, length)),
        vmem((heads, length)),
        vmem((1, heads)),
        vmem((1, heads)),
        vmem((length, heads * LANES)),
        vmem((length, width)),
        vmem((length, width)),
        pad,
        sems(18),
    ]
    (
        weighted, writes, reads, inside, conv, opened, head, xt, wt, rt, ct, scale, dt, rise, remain,
        rows_own, rims,
    ) = call(prepare_kernel, outs, ins, 18, scratch)
    before = lax.ppermute(rims, "sp", [(k, k + 1) for k in range(members - 1)])
    ins = (before, weighted, writes, reads, inside, conv, head, xt, wt, rt, ct, dt, rise, remain)
    outs = [sds((members, 16 + EXTRA, LANES), BF16), slim, full, side]
    payload, reads, inside, conv = call(state_kernel, outs, ins, 0, [pad])
    seqs = copies

    def moved(value, away):
        return lax.ppermute(value, "fs", [(k, (k + away) % seqs) for k in range(seqs)])

    rows_far = moved(rows_own, 2)
    gathered = lax.all_to_all(
        payload, "sp", 0, 0, axis_index_groups=turned(members, FIRST_OUT), tiled=True
    )
    prefixes = call(scan_kernel, [sds((members, 16, LANES), BF16)], (gathered,))[0]
    incoming = lax.all_to_all(prefixes, "sp", 0, 0, axis_index_groups=turned(members, FIRST_BACK), tiled=True)
    ins = (incoming, reads, rise, inside, opened, scale, conv)
    own = call(gate_kernel, [sds((length, width + wide), BF16)], ins, 0, [vmem((length, width))])[0]
    last = moved(own, 1)
    following = moved(own, -1)
    partial = call(far_kernel, [sds((length, rows_own.shape[1]), BF16)], (own, rows_far))[0]
    far = moved(partial, 2)
    swap = [(0, 1), (1, 0)]
    sent = part(False, True, own, far, rows_own)
    early_got = lax.ppermute(sent, "tp", swap)
    early = part(True, True, own, far, rows_own)
    sent = part(False, False, following, last, rows_own)
    late_got = lax.ppermute(sent, "tp", swap)
    late = part(True, False, following, last, rows_own)
    out = sds((2, length, rows_own.shape[1]), BF16)
    return call(merge_kernel, [out], (early, early_got, late, late_got))[0]


def solution(mesh):
    return jax.shard_map(
        per_device,
        mesh=mesh,
        in_specs=(
            P("fs", "sp", "tp"),
            P("fs", "sp", "tp"),
            P("fs", "sp", "tp"),
            P("fs", "sp", "tp"),
            P("fs", "sp", "tp"),
            P("tp"),
            P("tp"),
            P("sp", "tp"),
            P(None, "tp"),
            P(None, "tp"),
            P(None, "tp"),
            P("tp"),
            P("fs", "sp", "tp"),
            P("fs", "sp", "tp"),
            P("fs", "sp", "tp"),
            P(None, "tp"),
            P("tp", "fs"),
            P("tp", "fs"),
        ),
        out_specs=P("tp", "sp", "fs"),
        check_vma=False,
    )
```
